256 devices in a mesh: gr: 2 (over z_hi), fs: 16 (over z_lo, y), tp: 8 (over x, core).
Axes of the slice: x: 4, y: 4, z: 8 (z_hi: 2, z_lo: 4; z = z_hi * 4 + z_lo), core: 2. Of those that a mesh axis runs over, the one named last changes fastest.
Arguments:
- tokens: bfloat16 [32768, 2048], P(('gr', 'fs', 'tp')), may hold values from -6 to 6
- routes: int32 [32768, 8], P(('gr', 'fs', 'tp')), may hold values from 0 to 127, all different within a row; in each aligned block of 128 rows (0 to 127, 128 to 255, ...) at most 12 rows name the same one
- route_weights: float32 [32768, 8], P(('gr', 'fs', 'tp')), may hold values from 0.1 to 0.6
- norm_gain: float32 [2048], P(('gr', 'tp')), may hold values from 0.1 to 1.9
- gate_trained: float32 [128, 384, 2048], P(None, 'fs', ('gr', 'tp')), may hold values from -0.125 to 0.125
- up_trained: float32 [128, 384, 2048], P(None, 'fs', ('gr', 'tp')), may hold values from -0.125 to 0.125
- down_trained: float32 [128, 384, 2048], P(None, 'fs', ('gr', 'tp')), may hold values from -0.3125 to 0.3125
- shared_gate_trained: float32 [512, 2048], P('fs', ('gr', 'tp')), may hold values from -0.125 to 0.125
- shared_up_trained: float32 [512, 2048], P('fs', ('gr', 'tp')), may hold values from -0.125 to 0.125
- shared_down_trained: float32 [512, 2048], P('fs', ('gr', 'tp')), may hold values from -0.25 to 0.25
Outputs:
- combined: bfloat16 [32768, 2048], P(('gr', 'fs', 'tp'))
- expert_gate: bfloat16 [128, 384, 2048], P(('fs', 'tp'))
- expert_up: bfloat16 [128, 384, 2048], P(('fs', 'tp'))
- expert_down: bfloat16 [128, 384, 2048], P(('fs', 'tp'))
- shared_gate: bfloat16 [512, 2048], P('fs')
- shared_up: bfloat16 [512, 2048], P('fs')
- shared_down: bfloat16 [512, 2048], P('fs')
The draws below stay inside these ranges and needn't reach their ends.
Inputs may be any that keep to these rules, and one draw needn't show every extreme that they name: `routes`: each row names 8 different experts. Among the rows of one device no expert is named more than 12 times, and that many is reached in every draw.
All inputs are finite; a program needn't handle non-finite values.
Results may differ from the reference program's by a relative error of at most 0.0084.
Values may be sent and summed in bfloat16 or wider, within the bound.
No kernel may reach another device: no remote copies, remote signals or barrier semaphores. Data moves between devices by JAX's collectives and lax.ppermute only.
A program may use at most 128 MiB of HBM per device.

```python
import math
import jax
import jax.numpy as jnp
import numpy as np
from jax import lax

D = 2048
HE = 384
SH = 512
TOP_K = 8
TOK_DEV = 128
EXPERTS = 128
CAP = 12
TOKENS = 32768
N_GR = 2
N_FS = 16
N_TP = 8


def block_levels(rng, extent, split, smallest, largest):
    def one(axis_at, shards_of):
        steps = jax.random.uniform(jax.random.fold_in(jax.random.fold_in(rng, 6), axis_at), (shards_of,), jnp.float32, smallest / len(split), largest / len(split))
        return jnp.repeat(jnp.exp(steps), extent[axis_at] // shards_of).reshape((-1,) + (1,) * (len(extent) - axis_at - 1))

    factor_of = one(*split[0])
    for cut in split[1:]:
        factor_of = factor_of * one(*cut)
    return factor_of


def routed_block(key, own, number, rows, count, top, bound, lean):
    sequence = jax.random.permutation(key, count)
    crowded, common = shares(count, rows * top, bound, lean, True), shares(count, rows * top, bound, lean, False)
    places = jnp.arange(count)

    def named(tallies, turn):
        used = int((tallies > 0).sum())
        fixed = max(1, used // 4)
        passed = fixed + (places - fixed + turn * (used - fixed)) % max(1, count - fixed)
        return jnp.zeros((count,), jnp.int32).at[sequence[jnp.where(places < fixed, places, passed)]].set(jnp.asarray(tallies, jnp.int32))

    tallies = jnp.where(number % 4 == 0, named(crowded, number // 4), named(common, number - number // 4 - 1))
    mixed = jax.random.permutation(jax.random.fold_in(own, 3), count)
    source_of, receiver = mixed[0:count // 2 * 2:2], mixed[1:count // 2 * 2:2]
    margin = jnp.minimum(tallies[source_of] - 1, bound - tallies[receiver]) // 2
    margin = jnp.where((source_of == sequence[0]) | (receiver == sequence[0]) | (tallies[receiver] == 0), 0, jnp.maximum(margin, 0))
    passed = jax.random.randint(jax.random.fold_in(own, 4), (count // 2,), 0, 1 << 20) % (margin + 1)
    tallies = tallies.at[source_of].add(-passed).at[receiver].add(passed)
    members = jnp.searchsorted(jnp.cumsum(tallies), jnp.arange(rows * top), side="right").astype(jnp.int32)
    table = members.reshape(top, rows).T
    table = table[jax.random.permutation(jax.random.fold_in(own, 1), rows)]
    turn = jax.random.randint(jax.random.fold_in(own, 2), (rows, 1), 0, top)
    return jnp.take_along_axis(table, (jnp.arange(top)[None, :] + turn) % top, axis=1)


def shares(amount, total, most, lean, full):
    weights = [(1 << 20) // math.isqrt(rank ** lean) + 1 for rank in range(1, amount + 1)]
    largest = most if full else min(most, max(-(-total // amount), total * weights[0] // sum(weights)))
    least = 1 if total - largest >= amount - 1 else 0
    holding, rest = [largest] + [least] * (amount - 1), total - largest - least * (amount - 1)
    while rest > 0:
        candidates = [i for i in range(1, amount) if holding[i] < largest] or [i for i in range(1, amount) if holding[i] < most]
        pool, remaining = sum([weights[i] for i in candidates]), rest
        for i in candidates:
            more = min(most - holding[i], max(1, remaining * weights[i] // pool), rest)
            holding[i] = holding[i] + more
            rest = rest - more
    return np.array(holding)


def scatter_about(own_key, extent, scale, most, pieces=(), kind=jnp.bfloat16):
    drawn = jax.random.normal(own_key, extent, jnp.float32) * scale
    if len(pieces) > 0:
        drawn = block_levels(own_key, extent, pieces, -0.22, 0.18) * drawn
    return jnp.clip(drawn, min=-most, max=most).astype(kind)


def setup_inputs(seed: int = 0) -> dict:
    key_of = jax.random.split(jax.random.key(seed), 11)
    tokens = scatter_about(key_of[0], (TOKENS, D), 1.0, 6.0, ((0, 256),))
    routes_keys = jax.random.split(jax.random.fold_in(key_of[1], 1), TOKENS // TOK_DEV)
    routes_turns = jax.random.permutation(jax.random.fold_in(key_of[1], 3), TOKENS // TOK_DEV)
    routes = jax.vmap(lambda own, number: routed_block(jax.random.fold_in(key_of[1], 2), own, number, TOK_DEV, EXPERTS, TOP_K, CAP, 1))(routes_keys, routes_turns).reshape((TOKENS, TOP_K))
    route_weights = jnp.clip(0.1 + 0.5 * jax.random.uniform(key_of[2], (TOKENS, TOP_K), jnp.float32) ** block_levels(key_of[2], (TOKENS, TOP_K), ((0, 256),), -0.2, 0.2), 0.1, 0.6)
    norm_gain = jnp.clip(1.0 + 0.18 * jax.random.normal(key_of[3], (D,), jnp.float32), 0.1, 1.9)
    gate_trained = scatter_about(key_of[4], (EXPERTS, HE, D), D ** -0.5, 0.125, ((1, 16), (2, 16)), jnp.float32)
    up_trained = scatter_about(key_of[5], (EXPERTS, HE, D), D ** -0.5, 0.125, ((1, 16), (2, 16)), jnp.float32)
    down_trained = scatter_about(key_of[6], (EXPERTS, HE, D), HE ** -0.5, 0.3125, ((1, 16), (2, 16)), jnp.float32)
    shared_gate_trained = scatter_about(key_of[7], (SH, D), D ** -0.5, 0.125, ((0, 16), (1, 16)), jnp.float32)
    shared_up_trained = scatter_about(key_of[8], (SH, D), D ** -0.5, 0.125, ((0, 16), (1, 16)), jnp.float32)
    shared_down_trained = scatter_about(key_of[9], (SH, D), SH ** -0.5, 0.25, ((0, 16), (1, 16)), jnp.float32)
    return dict(tokens=tokens, routes=routes, route_weights=route_weights, norm_gain=norm_gain, gate_trained=gate_trained, up_trained=up_trained, down_trained=down_trained, shared_gate_trained=shared_gate_trained, shared_up_trained=shared_up_trained, shared_down_trained=shared_down_trained)


epsilon = 1e-06

def contract_rows(inputs, matrix):
    return lax.dot_general(inputs, matrix, (((1,), (1,)), ((), ())), preferred_element_type=jnp.float32)

def swiglu_rows(inputs, gate_matrix, up_matrix, down_matrix):
    hidden = (jax.nn.silu(contract_rows(inputs, gate_matrix)) * contract_rows(inputs, up_matrix)).astype(jnp.bfloat16)
    return jnp.dot(hidden, down_matrix, preferred_element_type=jnp.float32)

def reference(tokens, routes, route_weights, norm_gain, gate_trained, up_trained, down_trained, shared_gate_trained, shared_up_trained, shared_down_trained):
    expert_gate = (gate_trained * norm_gain[None, None, :]).astype(jnp.bfloat16)
    expert_up = (up_trained * norm_gain[None, None, :]).astype(jnp.bfloat16)
    expert_down = down_trained.astype(jnp.bfloat16)
    shared_gate = (shared_gate_trained * norm_gain[None, :]).astype(jnp.bfloat16)
    shared_up = (shared_up_trained * norm_gain[None, :]).astype(jnp.bfloat16)
    shared_down = shared_down_trained.astype(jnp.bfloat16)
    values = tokens.astype(jnp.float32)
    normed = (values * lax.rsqrt(lax.optimization_barrier(jnp.mean(values * values, axis=1, keepdims=True)) + epsilon)).astype(jnp.bfloat16)
    shared_out = swiglu_rows(normed, shared_gate, shared_up, shared_down)
    chosen = routes.reshape(-1).astype(jnp.int32)
    order = jnp.argsort(chosen, stable=True).astype(jnp.int32)
    sorted_tokens = (order // TOP_K).astype(jnp.int32)
    sorted_weights = route_weights.reshape(-1)[order]
    counts = jnp.bincount(chosen, length=EXPERTS).astype(jnp.int32)
    firsts = (jnp.cumsum(counts) - counts).astype(jnp.int32)
    limit = N_GR * N_FS * N_TP * CAP
    last_place = chosen.shape[0] - 1

    def per_expert(running, expert):
        offsets = jnp.arange(limit, dtype=jnp.int32)
        places = jnp.minimum(firsts[expert] + offsets, last_place).astype(jnp.int32)
        valid = offsets < counts[expert]
        rows_in = sorted_tokens[places]
        weights = jnp.where(valid, sorted_weights[places], jnp.zeros_like(sorted_weights[places]))
        result = swiglu_rows(normed[rows_in], expert_gate[expert], expert_up[expert], expert_down[expert]).astype(jnp.bfloat16)
        return (running.at[rows_in].add(weights[:, None] * result.astype(jnp.float32)), None)
    routed, _ = lax.scan(per_expert, jnp.zeros(tokens.shape, jnp.float32), jnp.arange(EXPERTS, dtype=jnp.int32))
    combined = (routed + shared_out).astype(jnp.bfloat16)
    return (combined, expert_gate, expert_up, expert_down, shared_gate, shared_up, shared_down)
```

```python
import functools

import jax
import jax.numpy as jnp
from jax import lax
from jax.experimental import pallas as pl
from jax.experimental.pallas import tpu as pltpu
from jax.sharding import Mesh, PartitionSpec as P

epsilon = 1e-06
ALL = ("gr", "zl", "y", "x", "c")
PLANE = ("y", "x", "c")
bf16 = jnp.bfloat16
f32 = jnp.float32


def swapped(array, axis, size, k):
    return lax.ppermute(array, axis, [(r, r ^ k) for r in range(size)])


def plane_exchange(array):
    return lax.all_to_all(array, PLANE, split_axis=0, concat_axis=0, tiled=True)


def ffn_rows(x, gate, up, down):
    contract = (((1,), (1,)), ((), ()))
    g = lax.dot_general(x, gate, contract, preferred_element_type=f32)
    u = lax.dot_general(x, up, contract, preferred_element_type=f32)
    hidden = (jax.nn.silu(g) * u).astype(bf16)
    return jnp.dot(hidden, down, preferred_element_type=f32)


def ffn_assemble_kernel(place, x, *refs, blocks, rows, cols):
    parts, refs = refs[:blocks], refs[blocks:]
    out, outs, held, sems = refs[0], refs[1:4], refs[4:7], refs[7]
    step = pl.program_id(0)

    def writes():
        return [
            pltpu.make_async_copy(held[m], outs[m].at[0], sems.at[blocks * 3 + m])
            for m in range(3)
        ]

    @pl.when(step == 0)
    def _():
        reads = []
        for k in range(blocks):
            row = pl.multiple_of(place[2 * k] * rows, rows)
            col = pl.multiple_of(place[2 * k + 1] * cols, cols)
            for m in range(3):
                reads.append(
                    pltpu.make_async_copy(
                        parts[k].at[m],
                        held[m].at[pl.ds(row, rows), pl.ds(col, cols)],
                        sems.at[k * 3 + m],
                    )
                )
        for r in reads:
            r.start()
        for r in reads:
            r.wait()
        for w in writes():
            w.start()

    out[...] = ffn_rows(x[...], held[0][...], held[1][...], held[2][...]).astype(bf16)

    @pl.when(step == pl.num_programs(0) - 1)
    def _():
        for w in writes():
            w.wait()


def ffn_assemble(place, x, parts, hidden, features, tile):
    count = x.shape[0]
    _, rows, cols = parts[0].shape
    matrix = jax.ShapeDtypeStruct((1, hidden, features), bf16)
    hbm = pl.BlockSpec(memory_space=pl.ANY)
    spec = pltpu.PrefetchScalarGridSpec(
        num_scalar_prefetch=1,
        grid=(count // tile,),
        in_specs=[pl.BlockSpec((tile, features), lambda i, p: (i, 0))] + [hbm] * len(parts),
        out_specs=[pl.BlockSpec((tile, features), lambda i, p: (i, 0))] + [hbm] * 3,
        scratch_shapes=[pltpu.VMEM((hidden, features), bf16)] * 3
        + [pltpu.SemaphoreType.DMA((len(parts) * 3 + 3,))],
    )
    return pl.pallas_call(
        functools.partial(ffn_assemble_kernel, blocks=len(parts), rows=rows, cols=cols),
        grid_spec=spec,
        out_shape=[jax.ShapeDtypeStruct((count, features), bf16)] + [matrix] * 3,
        cost_estimate=pl.CostEstimate(
            flops=6 * count * hidden * features,
            bytes_accessed=4 * count * features + 12 * hidden * features,
            transcendentals=count * hidden,
        ),
        name="ffn_assemble",
    )(place, x, *parts)


def ffn_kernel(x, gate, up, down, out):
    out[...] = ffn_rows(x[...], gate[0], up[0], down[0]).astype(bf16)


def ffn(x, gate, up, down, tile):
    count, features = x.shape
    hidden = gate.shape[1]
    whole = pl.BlockSpec((1, hidden, features), lambda i: (0, 0, 0))
    rows = pl.BlockSpec((tile, features), lambda i: (i, 0))
    return pl.pallas_call(
        ffn_kernel,
        grid=(count // tile,),
        in_specs=[rows, whole, whole, whole],
        out_specs=rows,
        out_shape=jax.ShapeDtypeStruct((count, features), bf16),
        cost_estimate=pl.CostEstimate(
            flops=6 * count * hidden * features,
            bytes_accessed=4 * count * features + 6 * hidden * features,
            transcendentals=count * hidden,
        ),
        name="ffn_rows",
    )(x, gate, up, down)


def selection(metas, first, experts, top, capacity):
    codes, weights = [], []
    for k, meta in enumerate(metas):
        names = meta[:top] - first.astype(f32)
        hits = names[:, None, :] == jnp.arange(experts, dtype=f32)[None, :, None]
        chosen = jnp.sum(hits.astype(f32), axis=0)
        weight = jnp.sum(jnp.where(hits, meta[top:, None, :], 0.0), axis=0)
        n = chosen.shape[1]
        before = (jnp.arange(n)[:, None] < jnp.arange(n)[None, :]).astype(bf16)
        place = jnp.dot(chosen.astype(bf16), before, preferred_element_type=f32)
        codes.append(jnp.where(chosen > 0, place + float(k * capacity), -1.0))
        weights.append(weight)
    code = jnp.concatenate(codes, axis=1).astype(bf16)
    weight = jnp.concatenate(weights, axis=1)
    high = weight.astype(bf16)
    low = (weight - high.astype(f32)).astype(bf16)
    span = len(metas) * capacity
    slot = jnp.arange(experts * span, dtype=jnp.int32)
    spread = (slot[:, None] // span == jnp.arange(experts, dtype=jnp.int32)[None, :]).astype(bf16)
    hit = jnp.dot(spread, code, preferred_element_type=f32) == (slot % span).astype(f32)[:, None]
    pick = hit.astype(bf16)
    high = jnp.where(hit, jnp.dot(spread, high, preferred_element_type=f32), 0.0).astype(bf16)
    low = jnp.where(hit, jnp.dot(spread, low, preferred_element_type=f32), 0.0).astype(bf16)
    return pick, high, low


def from_slots(matrix, rows):
    return lax.dot_general(matrix, rows, (((0,), (0,)), ((), ())), preferred_element_type=f32)


def body(
    tokens,
    routes,
    route_weights,
    norm_gain,
    gate_trained,
    up_trained,
    down_trained,
    shared_gate_trained,
    shared_up_trained,
    shared_down_trained,
):
    gr, zl, y = (lax.axis_index(a) for a in ("gr", "zl", "y"))
    n_gr, n_zl, n_y = (lax.axis_size(a) for a in ("gr", "zl", "y"))
    n_xc = lax.axis_size("x") * lax.axis_size("c")
    n_plane = n_y * n_xc
    row_count, features = tokens.shape
    top = routes.shape[1]
    experts, own_hidden, own_cols = gate_trained.shape
    capacity = max(2, 3 * row_count * top // (2 * experts))

    meta = jnp.concatenate([routes.T.astype(f32), route_weights.T], axis=0)
    metas = [meta] + [swapped(meta, "zl", n_zl, k) for k in range(1, n_zl)]
    values = tokens.astype(f32)
    normed = (
        values * lax.rsqrt(jnp.mean(values * values, axis=1, keepdims=True) + epsilon)
    ).astype(bf16)
    blocks = [normed] + [swapped(normed, "zl", n_zl, k) for k in range(1, n_zl)]

    gain = norm_gain[None, :]
    shared = jnp.stack(
        [shared_gate_trained * gain, shared_up_trained * gain, shared_down_trained], axis=0
    ).astype(bf16)
    other = swapped(shared, "gr", n_gr, 1)
    shared = jnp.where(gr == 0, jnp.stack([shared, other]), jnp.stack([other, shared]))

    gain = norm_gain[None, None, :]
    stacked = jnp.stack(
        [gate_trained * gain, up_trained * gain, down_trained], axis=1
    ).astype(bf16)
    stacked = stacked.reshape(n_zl, n_plane, 3, own_hidden, own_cols)
    ordered = [
        lax.dynamic_index_in_dim(stacked, zl ^ j, 0, keepdims=False) for j in range(n_zl)
    ]
    sent = jnp.stack(ordered, axis=1).reshape(n_plane, n_zl * 3 * own_hidden, own_cols)
    extra = jnp.broadcast_to(
        shared.reshape(1, -1, own_cols), (n_plane, shared.size // own_cols, own_cols)
    )
    landed = plane_exchange(jnp.concatenate([sent, extra], axis=1))
    count = n_zl * 3 * own_hidden
    moved = landed[:, :count].reshape(n_y, n_xc, n_zl, 3, own_hidden, own_cols)
    moved = [
        moved[:, :, j].transpose(2, 0, 3, 1, 4).reshape(3, n_y * own_hidden, n_xc * own_cols)
        for j in range(n_zl)
    ]
    parts = [
        moved[k % n_zl]
        if k == 0
        else swapped(moved[k % n_zl], ("gr", "zl"), n_gr * n_zl, k)
        for k in range(n_gr * n_zl)
    ]
    place = jnp.stack(
        [v for k in range(n_gr * n_zl) for v in (zl ^ (k % n_zl), gr ^ (k // n_zl))]
    ).astype(jnp.int32)

    share = shared.shape[2]
    quarter = landed[:, count:].reshape(n_y, n_xc, n_gr, 3, share, own_cols)
    quarter = quarter.transpose(3, 0, 4, 2, 1, 5).reshape(3, n_y * share, features)
    shared_out = [
        lax.dynamic_slice_in_dim(quarter[m], y * share, share, axis=0) for m in range(3)
    ]

    first = zl * n_plane
    near_picks = selection(metas[:2], first, n_plane, top, capacity)
    far_picks = selection(metas[2:], first, n_plane, top, capacity)
    near_tokens = jnp.concatenate(blocks[:2], axis=0)
    far_tokens = jnp.concatenate(blocks[2:], axis=0)

    def dispatched(pick, rows):
        out = jnp.dot(pick, rows, preferred_element_type=f32).astype(bf16)
        out = plane_exchange(out.reshape(n_plane, 2 * capacity, features))
        return out.reshape(-1, features)

    near_in = dispatched(near_picks[0], near_tokens)
    far_in = dispatched(far_picks[0], far_tokens)

    def shared_part(rows):
        contract = (((1,), (1,)), ((), ()))
        g = lax.dot_general(rows, quarter[0], contract, preferred_element_type=f32)
        u = lax.dot_general(rows, quarter[1], contract, preferred_element_type=f32)
        hidden = (jax.nn.silu(g) * u).astype(bf16)
        return jnp.dot(hidden, quarter[2], preferred_element_type=f32)

    far_shared = shared_part(far_tokens)
    near_shared = shared_part(near_tokens)

    hidden = own_hidden * n_zl * n_y
    far_result, expert_gate, expert_up, expert_down = ffn_assemble(
        place, far_in, parts, hidden, features, 256
    )
    far_back = plane_exchange(far_result.reshape(n_plane, 2 * capacity, features))
    near_result = ffn(near_in, expert_gate, expert_up, expert_down, 256)
    near_back = plane_exchange(near_result.reshape(n_plane, 2 * capacity, features))

    def gathered(picks, back, extra):
        back = back.reshape(-1, features)
        return from_slots(picks[1], back) + from_slots(picks[2], back) + extra

    far_sum = gathered(far_picks, far_back, far_shared).astype(bf16)
    third = swapped(far_sum[:row_count], "zl", n_zl, 2)
    fourth = swapped(far_sum[row_count:], "zl", n_zl, 3)
    near_sum = gathered(near_picks, near_back, near_shared)
    second = swapped(near_sum[row_count:].astype(bf16), "zl", n_zl, 1)
    combined = (
        near_sum[:row_count] + second.astype(f32) + third.astype(f32) + fourth.astype(f32)
    ).astype(bf16)
    return (combined, expert_gate, expert_up, expert_down, *shared_out)


def solution(mesh):
    fine = Mesh(mesh.devices.reshape(2, 4, 4, 4, 2), ALL)
    cols = ("gr", "x", "c")
    in_specs = (
        P(ALL, None),
        P(ALL, None),
        P(ALL, None),
        P(cols),
        P(None, ("zl", "y"), cols),
        P(None, ("zl", "y"), cols),
        P(None, ("zl", "y"), cols),
        P(("zl", "y"), cols),
        P(("zl", "y"), cols),
        P(("zl", "y"), cols),
    )
    out_specs = (
        P(ALL, None),
        P(("zl", "y", "x", "c"), None, None),
        P(("zl", "y", "x", "c"), None, None),
        P(("zl", "y", "x", "c"), None, None),
        P(("zl", "y"), None),
        P(("zl", "y"), None),
        P(("zl", "y"), None),
    )
    return jax.shard_map(body, mesh=fine, in_specs=in_specs, out_specs=out_specs, check_vma=False)
```

```python
import functools

import jax
import jax.numpy as jnp
from jax import lax
from jax.experimental import pallas as pl
from jax.experimental.pallas import tpu as pltpu
from jax.sharding import Mesh, PartitionSpec as P

epsilon = 1e-06
ALL = ("gr", "zl", "y", "x", "c")
PLANE = ("y", "x", "c")
bf16 = jnp.bfloat16
f32 = jnp.float32


def swapped(array, axis, size, k):
    return lax.ppermute(array, axis, [(r, r ^ k) for r in range(size)])


def plane_exchange(array):
    return lax.all_to_all(array, PLANE, split_axis=0, concat_axis=0, tiled=True)


def ffn_rows(x, gate, up, down):
    contract = (((1,), (1,)), ((), ()))
    g = lax.dot_general(x, gate, contract, preferred_element_type=f32)
    u = lax.dot_general(x, up, contract, preferred_element_type=f32)
    hidden = (jax.nn.silu(g) * u).astype(bf16)
    return jnp.dot(hidden, down, preferred_element_type=f32)


def cast_kernel(place, gain, gate, up, down, out):
    n = gate.shape[1]
    scale = gain[...][None]
    out[:, :n, :] = (gate[...] * scale).astype(bf16)
    out[:, n : 2 * n, :] = (up[...] * scale).astype(bf16)
    out[:, 2 * n :, :] = down[...].astype(bf16)


def cast(place, gain, gate, up, down, n_plane):
    experts, n, cols = gate.shape
    n_zl = experts // n_plane
    piece = pl.BlockSpec((n_plane, n, cols), lambda j, p: (p[0] ^ j, 0, 0))
    spec = pltpu.PrefetchScalarGridSpec(
        num_scalar_prefetch=1,
        grid=(n_zl,),
        in_specs=[pl.BlockSpec((1, cols), lambda j, p: (0, 0)), piece, piece, piece],
        out_specs=pl.BlockSpec((n_plane, 3 * n, cols), lambda j, p: (0, j, 0)),
    )
    return pl.pallas_call(
        cast_kernel,
        grid_spec=spec,
        out_shape=jax.ShapeDtypeStruct((n_plane, n_zl * 3 * n, cols), bf16),
        cost_estimate=pl.CostEstimate(
            flops=3 * gate.size, bytes_accessed=18 * gate.size, transcendentals=0
        ),
        name="cast",
    )(place, gain, gate, up, down)


def ffn_assemble_kernel(place, x, *refs, blocks, n_y, n_xc, own_hidden, cols):
    parts, refs = refs[:blocks], refs[blocks:]
    out, outs, held, sems = refs[0], refs[1:4], refs[4:7], refs[7]
    step = pl.program_id(0)
    n_cols = held[0].shape[0]

    def writes():
        return [
            pltpu.make_async_copy(
                held[m].at[f],
                outs[m].at[0, :, pl.ds(f * cols, cols)],
                sems.at[blocks * 3 * n_y + m * n_cols + f],
            )
            for m in range(3)
            for f in range(n_cols)
        ]

    @pl.when(step == 0)
    def _():
        reads = []
        for k in range(blocks):
            row = place[2 * k] * (n_y * own_hidden)
            col = place[2 * k + 1] * n_xc
            for m in range(3):
                for y in range(n_y):
                    at = pl.multiple_of(row + y * own_hidden, 8)
                    reads.append(
                        pltpu.make_async_copy(
                            parts[k].at[pl.ds(y * n_xc, n_xc), pl.ds(m * own_hidden, own_hidden)],
                            held[m].at[pl.ds(col, n_xc), pl.ds(at, own_hidden)],
                            sems.at[(k * 3 + m) * n_y + y],
                        )
                    )
        for r in reads:
            r.start()
        for r in reads:
            r.wait()
        for w in writes():
            w.start()

    gate, up, down = (
        jnp.concatenate([held[m][f] for f in range(n_cols)], axis=1) for m in range(3)
    )
    out[...] = ffn_rows(x[...], gate, up, down).astype(bf16)

    @pl.when(step == pl.num_programs(0) - 1)
    def _():
        for w in writes():
            w.wait()


def ffn_assemble(place, x, parts, n_y, n_xc, own_hidden, tile):
    count, features = x.shape
    cols = parts[0].shape[2]
    n_cols = features // cols
    hidden = len(parts) * n_y * n_xc * own_hidden * cols // features
    matrix = jax.ShapeDtypeStruct((1, hidden, features), bf16)
    hbm = pl.BlockSpec(memory_space=pl.ANY)
    spec = pltpu.PrefetchScalarGridSpec(
        num_scalar_prefetch=1,
        grid=(count // tile,),
        in_specs=[pl.BlockSpec((tile, features), lambda i, p: (i, 0))] + [hbm] * len(parts),
        out_specs=[pl.BlockSpec((tile, features), lambda i, p: (i, 0))] + [hbm] * 3,
        scratch_shapes=[pltpu.VMEM((n_cols, hidden, cols), bf16)] * 3
        + [pltpu.SemaphoreType.DMA((len(parts) * 3 * n_y + 3 * n_cols,))],
    )
    return pl.pallas_call(
        functools.partial(
            ffn_assemble_kernel,
            blocks=len(parts),
            n_y=n_y,
            n_xc=n_xc,
            own_hidden=own_hidden,
            cols=cols,
        ),
        grid_spec=spec,
        out_shape=[jax.ShapeDtypeStruct((count, features), bf16)] + [matrix] * 3,
        cost_estimate=pl.CostEstimate(
            flops=6 * count * hidden * features,
            bytes_accessed=4 * count * features + 12 * hidden * features,
            transcendentals=count * hidden,
        ),
        name="ffn_assemble",
    )(place, x, *parts)


def ffn_kernel(x, gate, up, down, out):
    out[...] = ffn_rows(x[...], gate[0], up[0], down[0]).astype(bf16)


def ffn(x, gate, up, down, tile):
    count, features = x.shape
    hidden = gate.shape[1]
    whole = pl.BlockSpec((1, hidden, features), lambda i: (0, 0, 0))
    rows = pl.BlockSpec((tile, features), lambda i: (i, 0))
    return pl.pallas_call(
        ffn_kernel,
        grid=(count // tile,),
        in_specs=[rows, whole, whole, whole],
        out_specs=rows,
        out_shape=jax.ShapeDtypeStruct((count, features), bf16),
        cost_estimate=pl.CostEstimate(
            flops=6 * count * hidden * features,
            bytes_accessed=4 * count * features + 6 * hidden * features,
            transcendentals=count * hidden,
        ),
        name="ffn_rows",
    )(x, gate, up, down)


def selection(metas, first, experts, top, capacity):
    codes, weights = [], []
    for k, meta in enumerate(metas):
        names = meta[:top] - first.astype(f32)
        hits = names[:, None, :] == jnp.arange(experts, dtype=f32)[None, :, None]
        chosen = jnp.sum(hits.astype(f32), axis=0)
        weight = jnp.sum(jnp.where(hits, meta[top:, None, :], 0.0), axis=0)
        n = chosen.shape[1]
        before = (jnp.arange(n)[:, None] < jnp.arange(n)[None, :]).astype(bf16)
        place = jnp.dot(chosen.astype(bf16), before, preferred_element_type=f32)
        codes.append(jnp.where(chosen > 0, place + float(k * capacity), -1.0))
        weights.append(weight)
    code = jnp.concatenate(codes, axis=1).astype(bf16)
    weight = jnp.concatenate(weights, axis=1)
    high = weight.astype(bf16)
    low = (weight - high.astype(f32)).astype(bf16)
    span = len(metas) * capacity
    slot = jnp.arange(experts * span, dtype=jnp.int32)
    within = (slot % span).astype(f32)
    spread = (slot[:, None] // span == jnp.arange(experts, dtype=jnp.int32)[None, :]).astype(bf16)
    pick = jnp.dot(spread, code, preferred_element_type=f32) == within[:, None]

    def by_token(values):
        return lax.dot_general(
            values, spread, (((0,), (1,)), ((), ())), preferred_element_type=f32
        )

    held = by_token(code) == within[None, :]
    high = jnp.where(held, by_token(high), 0.0).astype(bf16)
    low = jnp.where(held, by_token(low), 0.0).astype(bf16)
    return pick.astype(bf16), high, low


def combine_kernel(high, low, back, hidden, down, out):
    rows = back[...]
    total = jnp.dot(high[...], rows, preferred_element_type=f32)
    total += jnp.dot(low[...], rows, preferred_element_type=f32)
    total += jnp.dot(hidden[...], down[...], preferred_element_type=f32)
    out[...] = total.astype(out.dtype)


def combine(high, low, back, hidden, down, dtype, tile):
    count, slots = high.shape
    features = back.shape[1]
    units = hidden.shape[1]
    whole = lambda *shape: pl.BlockSpec(shape, lambda i: (0, 0))
    part = lambda rows: pl.BlockSpec((rows, tile), lambda i: (0, i))
    return pl.pallas_call(
        combine_kernel,
        grid=(features // tile,),
        in_specs=[
            whole(count, slots),
            whole(count, slots),
            part(slots),
            whole(count, units),
            part(units),
        ],
        out_specs=part(count),
        out_shape=jax.ShapeDtypeStruct((count, features), dtype),
        cost_estimate=pl.CostEstimate(
            flops=2 * count * features * (2 * slots + units),
            bytes_accessed=4 * count * slots + 2 * slots * features + 4 * count * features,
            transcendentals=0,
        ),
        name="combine",
    )(high, low, back, hidden, down)


def body(
    tokens,
    routes,
    route_weights,
    norm_gain,
    gate_trained,
    up_trained,
    down_trained,
    shared_gate_trained,
    shared_up_trained,
    shared_down_trained,
):
    gr, zl, y = (lax.axis_index(a) for a in ("gr", "zl", "y"))
    n_gr, n_zl, n_y = (lax.axis_size(a) for a in ("gr", "zl", "y"))
    n_xc = lax.axis_size("x") * lax.axis_size("c")
    n_plane = n_y * n_xc
    row_count, features = tokens.shape
    top = routes.shape[1]
    experts, own_hidden, own_cols = gate_trained.shape
    capacity = max(2, 3 * row_count * top // (2 * experts))

    meta = jnp.concatenate([routes.T.astype(f32), route_weights.T], axis=0)
    metas = [meta] + [swapped(meta, "zl", n_zl, k) for k in range(1, n_zl)]
    values = tokens.astype(f32)
    normed = (
        values * lax.rsqrt(jnp.mean(values * values, axis=1, keepdims=True) + epsilon)
    ).astype(bf16)
    blocks = [normed] + [swapped(normed, "zl", n_zl, k) for k in range(1, n_zl)]

    gain = norm_gain[None, :]
    shared = jnp.stack(
        [shared_gate_trained * gain, shared_up_trained * gain, shared_down_trained], axis=0
    ).astype(bf16)
    other = swapped(shared, "gr", n_gr, 1)
    shared = jnp.where(gr == 0, jnp.stack([shared, other]), jnp.stack([other, shared]))

    steps = range(n_gr * n_zl)
    place = jnp.stack([v for k in steps for v in (zl ^ (k % n_zl), gr ^ (k // n_zl))])
    place = place.astype(jnp.int32)
    sent = cast(place, norm_gain[None, :], gate_trained, up_trained, down_trained, n_plane)
    landed = plane_exchange(sent)
    piece = 3 * own_hidden
    moved = [landed[:, j * piece : (j + 1) * piece] for j in range(n_zl)]
    parts = [moved[0]] + [
        swapped(moved[k % n_zl], ("gr", "zl"), n_gr * n_zl, k) for k in steps[1:]
    ]

    first = zl * n_plane
    near_picks = selection(metas[:2], first, n_plane, top, capacity)
    far_picks = selection(metas[2:], first, n_plane, top, capacity)
    near_tokens = jnp.concatenate(blocks[:2], axis=0)
    far_tokens = jnp.concatenate(blocks[2:], axis=0)

    def dispatched(pick, rows, after):
        out = jnp.dot(pick, rows, preferred_element_type=f32).astype(bf16)
        out, _ = lax.optimization_barrier((out, after))
        return plane_exchange(out.reshape(n_plane, 2 * capacity, features))

    near_in = dispatched(near_picks[0], near_tokens, landed)
    far_in = dispatched(far_picks[0], far_tokens, near_in)

    share = shared.shape[2]
    extra = jnp.broadcast_to(
        shared.reshape(1, -1, own_cols), (n_plane, shared.size // own_cols, own_cols)
    )
    extra, _ = lax.optimization_barrier((extra, far_in))
    quarter = plane_exchange(extra).reshape(n_y, n_xc, n_gr, 3, share, own_cols)
    quarter = quarter.transpose(3, 0, 4, 2, 1, 5).reshape(3, n_y * share, features)
    shared_out = [
        lax.dynamic_slice_in_dim(quarter[m], y * share, share, axis=0) for m in range(3)
    ]

    def shared_hidden(rows):
        contract = (((1,), (1,)), ((), ()))
        g = lax.dot_general(rows, quarter[0], contract, preferred_element_type=f32)
        u = lax.dot_general(rows, quarter[1], contract, preferred_element_type=f32)
        return (jax.nn.silu(g) * u).astype(bf16)

    near_hidden = shared_hidden(near_tokens)
    far_hidden = shared_hidden(far_tokens)
    shared_down = quarter[2]
    far_in, near_hidden, far_hidden, shared_down = lax.optimization_barrier(
        (far_in, near_hidden, far_hidden, shared_down)
    )

    far_result, expert_gate, expert_up, expert_down = ffn_assemble(
        place, far_in.reshape(-1, features), parts, n_y, n_xc, own_hidden, 256
    )
    far_back = plane_exchange(far_result.reshape(n_plane, 2 * capacity, features))
    near_result = ffn(near_in.reshape(-1, features), expert_gate, expert_up, expert_down, 256)
    near_back = plane_exchange(near_result.reshape(n_plane, 2 * capacity, features))

    far_sum = combine(
        *far_picks[1:], far_back.reshape(-1, features), far_hidden, shared_down, bf16, 512
    )
    third = swapped(far_sum[:row_count], "zl", n_zl, 2)
    fourth = swapped(far_sum[row_count:], "zl", n_zl, 3)
    near_sum = combine(
        *near_picks[1:], near_back.reshape(-1, features), near_hidden, shared_down, f32, 512
    )
    second = swapped(near_sum[row_count:].astype(bf16), "zl", n_zl, 1)
    combined = (
        near_sum[:row_count] + second.astype(f32) + third.astype(f32) + fourth.astype(f32)
    ).astype(bf16)
    return (combined, expert_gate, expert_up, expert_down, *shared_out)


def solution(mesh):
    fine = Mesh(mesh.devices.reshape(2, 4, 4, 4, 2), ALL)
    cols = ("gr", "x", "c")
    in_specs = (
        P(ALL, None),
        P(ALL, None),
        P(ALL, None),
        P(cols),
        P(None, ("zl", "y"), cols),
        P(None, ("zl", "y"), cols),
        P(None, ("zl", "y"), cols),
        P(("zl", "y"), cols),
        P(("zl", "y"), cols),
        P(("zl", "y"), cols),
    )
    out_specs = (
        P(ALL, None),
        P(("zl", "y", "x", "c"), None, None),
        P(("zl", "y", "x", "c"), None, None),
        P(("zl", "y", "x", "c"), None, None),
        P(("zl", "y"), None),
        P(("zl", "y"), None),
        P(("zl", "y"), None),
    )
    return jax.shard_map(body, mesh=fine, in_specs=in_specs, out_specs=out_specs, check_vma=False)
```

```python
import functools

import jax
import jax.numpy as jnp
from jax import lax
from jax.experimental import pallas as pl
from jax.experimental.pallas import tpu as pltpu
from jax.sharding import Mesh, PartitionSpec as P


epsilon = 1e-06
ALL = ("gr", "zl", "y", "x", "c")
PLANE = ("y", "x", "c")
bf16 = jnp.bfloat16
f32 = jnp.float32


def swapped(array, axis, size, k):
    return lax.ppermute(array, axis, [(r, r ^ k) for r in range(size)])


def plane_exchange(array):
    return lax.all_to_all(array, PLANE, split_axis=0, concat_axis=0, tiled=True)


def ffn_rows(x, gate, up, down):
    contract = (((1,), (1,)), ((), ()))
    g = lax.dot_general(x, gate, contract, preferred_element_type=f32)
    u = lax.dot_general(x, up, contract, preferred_element_type=f32)
    hidden = (jax.nn.silu(g) * u).astype(bf16)
    return jnp.dot(hidden, down, preferred_element_type=f32)


def cast_kernel(place, gain, gate, up, down, out):
    n = gate.shape[1]
    scale = gain[...][None]
    out[:, :n, :] = (gate[...] * scale).astype(bf16)
    out[:, n : 2 * n, :] = (up[...] * scale).astype(bf16)
    out[:, 2 * n :, :] = down[...].astype(bf16)


def cast(place, gain, gate, up, down, n_plane):
    experts, n, cols = gate.shape
    n_zl = experts // n_plane
    piece = pl.BlockSpec((n_plane, n, cols), lambda j, p: (p[0] ^ j, 0, 0))
    spec = pltpu.PrefetchScalarGridSpec(
        num_scalar_prefetch=1,
        grid=(n_zl,),
        in_specs=[pl.BlockSpec((1, cols), lambda j, p: (0, 0)), piece, piece, piece],
        out_specs=pl.BlockSpec((n_plane, 3 * n, cols), lambda j, p: (0, j, 0)),
    )
    return pl.pallas_call(
        cast_kernel,
        grid_spec=spec,
        out_shape=jax.ShapeDtypeStruct((n_plane, n_zl * 3 * n, cols), bf16),
        cost_estimate=pl.CostEstimate(
            flops=3 * gate.size, bytes_accessed=18 * gate.size, transcendentals=0
        ),
        name="cast",
    )(place, gain, gate, up, down)


def ffn_assemble_kernel(place, x, *refs, blocks, n_y, n_xc, own_hidden, cols):
    parts, refs = refs[:blocks], refs[blocks:]
    out, outs, held, sems = refs[0], refs[1:4], refs[4:7], refs[7]
    step = pl.program_id(0)
    n_cols = held[0].shape[0]

    def writes():
        return [
            pltpu.make_async_copy(
                held[m].at[f],
                outs[m].at[0, :, pl.ds(f * cols, cols)],
                sems.at[blocks * 3 * n_y + m * n_cols + f],
            )
            for m in range(3)
            for f in range(n_cols)
        ]

    @pl.when(step == 0)
    def _():
        reads = []
        for k in range(blocks):
            row = place[2 * k] * (n_y * own_hidden)
            col = place[2 * k + 1] * n_xc
            for m in range(3):
                for y in range(n_y):
                    at = pl.multiple_of(row + y * own_hidden, 8)
                    reads.append(
                        pltpu.make_async_copy(
                            parts[k].at[pl.ds(y * n_xc, n_xc), pl.ds(m * own_hidden, own_hidden)],
                            held[m].at[pl.ds(col, n_xc), pl.ds(at, own_hidden)],
                            sems.at[(k * 3 + m) * n_y + y],
                        )
                    )
        for r in reads:
            r.start()
        for r in reads:
            r.wait()
        for w in writes():
            w.start()

    gate, up, down = (
        jnp.concatenate([held[m][f] for f in range(n_cols)], axis=1) for m in range(3)
    )
    out[...] = ffn_rows(x[...], gate, up, down).astype(bf16)

    @pl.when(step == pl.num_programs(0) - 1)
    def _():
        for w in writes():
            w.wait()


def ffn_assemble(place, x, parts, n_y, n_xc, own_hidden, tile):
    count, features = x.shape
    cols = parts[0].shape[2]
    n_cols = features // cols
    hidden = len(parts) * n_y * n_xc * own_hidden * cols // features
    matrix = jax.ShapeDtypeStruct((1, hidden, features), bf16)
    hbm = pl.BlockSpec(memory_space=pl.ANY)
    spec = pltpu.PrefetchScalarGridSpec(
        num_scalar_prefetch=1,
        grid=(count // tile,),
        in_specs=[pl.BlockSpec((tile, features), lambda i, p: (i, 0))] + [hbm] * len(parts),
        out_specs=[pl.BlockSpec((tile, features), lambda i, p: (i, 0))] + [hbm] * 3,
        scratch_shapes=[pltpu.VMEM((n_cols, hidden, cols), bf16)] * 3
        + [pltpu.SemaphoreType.DMA((len(parts) * 3 * n_y + 3 * n_cols,))],
    )
    return pl.pallas_call(
        functools.partial(
            ffn_assemble_kernel,
            blocks=len(parts),
            n_y=n_y,
            n_xc=n_xc,
            own_hidden=own_hidden,
            cols=cols,
        ),
        grid_spec=spec,
        out_shape=[jax.ShapeDtypeStruct((count, features), bf16)] + [matrix] * 3,
        cost_estimate=pl.CostEstimate(
            flops=6 * count * hidden * features,
            bytes_accessed=4 * count * features + 12 * hidden * features,
            transcendentals=count * hidden,
        ),
        name="ffn_assemble",
    )(place, x, *parts)


def ffn_kernel(x, gate, up, down, out):
    out[...] = ffn_rows(x[...], gate[0], up[0], down[0]).astype(bf16)


def ffn(x, gate, up, down, tile):
    count, features = x.shape
    hidden = gate.shape[1]
    whole = pl.BlockSpec((1, hidden, features), lambda i: (0, 0, 0))
    rows = pl.BlockSpec((tile, features), lambda i: (i, 0))
    return pl.pallas_call(
        ffn_kernel,
        grid=(count // tile,),
        in_specs=[rows, whole, whole, whole],
        out_specs=rows,
        out_shape=jax.ShapeDtypeStruct((count, features), bf16),
        cost_estimate=pl.CostEstimate(
            flops=6 * count * hidden * features,
            bytes_accessed=4 * count * features + 6 * hidden * features,
            transcendentals=count * hidden,
        ),
        name="ffn_rows",
    )(x, gate, up, down)


def selection(metas, first, experts, top, capacity):
    codes, weights = [], []
    for k, meta in enumerate(metas):
        names = meta[:top] - first.astype(f32)
        hits = names[:, None, :] == jnp.arange(experts, dtype=f32)[None, :, None]
        chosen = jnp.sum(hits.astype(f32), axis=0)
        weight = jnp.sum(jnp.where(hits, meta[top:, None, :], 0.0), axis=0)
        n = chosen.shape[1]
        before = (jnp.arange(n)[:, None] < jnp.arange(n)[None, :]).astype(bf16)
        place = jnp.dot(chosen.astype(bf16), before, preferred_element_type=f32)
        codes.append(jnp.where(chosen > 0, place + float(k * capacity), -1.0))
        weights.append(weight)
    code = jnp.concatenate(codes, axis=1).astype(bf16)
    weight = jnp.concatenate(weights, axis=1)
    high = weight.astype(bf16)
    low = (weight - high.astype(f32)).astype(bf16)
    span = len(metas) * capacity
    slot = jnp.arange(experts * span, dtype=jnp.int32)
    within = (slot % span).astype(f32)
    spread = (slot[:, None] // span == jnp.arange(experts, dtype=jnp.int32)[None, :]).astype(bf16)

    def by_token(values):
        return lax.dot_general(
            values, spread, (((0,), (1,)), ((), ())), preferred_element_type=f32
        )

    held = by_token(code) == within[None, :]
    high = jnp.where(held, by_token(high), 0.0).astype(bf16)
    low = jnp.where(held, by_token(low), 0.0).astype(bf16)
    return code, high, low


def pick_kernel(code, one, two, out, *, span, tile):
    slot = lax.broadcasted_iota(jnp.int32, (tile, 1), 0) + pl.program_id(0) * tile
    expert = slot // span
    within = (slot - expert * span).astype(f32)
    names = lax.broadcasted_iota(jnp.int32, (tile, code.shape[0]), 1)
    spread = (names == expert).astype(f32).astype(bf16)
    held = jnp.dot(spread, code[...], preferred_element_type=f32) == within
    held = held.astype(f32).astype(bf16)
    n = one.shape[0]
    total = jnp.dot(held[:, :n], one[...], preferred_element_type=f32)
    total += jnp.dot(held[:, n:], two[...], preferred_element_type=f32)
    out[...] = total.astype(bf16)


def pick(code, one, two, span, tile):
    experts, count = code.shape
    features = one.shape[1]
    slots = experts * span
    whole = lambda a: pl.BlockSpec(a.shape, lambda i: (0, 0))
    return pl.pallas_call(
        functools.partial(pick_kernel, span=span, tile=tile),
        grid=(slots // tile,),
        in_specs=[whole(code), whole(one), whole(two)],
        out_specs=pl.BlockSpec((tile, features), lambda i: (i, 0)),
        out_shape=jax.ShapeDtypeStruct((slots, features), bf16),
        cost_estimate=pl.CostEstimate(
            flops=2 * slots * count * features,
            bytes_accessed=2 * (slots + count) * features,
            transcendentals=0,
        ),
        name="pick",
    )(code, one, two)


def combine_kernel(high, low, back, hidden, down, out):
    rows = back[...]
    total = jnp.dot(high[...], rows, preferred_element_type=f32)
    total += jnp.dot(low[...], rows, preferred_element_type=f32)
    total += jnp.dot(hidden[...], down[...], preferred_element_type=f32)
    out[...] = total.astype(out.dtype)


def combine(high, low, back, hidden, down, dtype, tile):
    count, slots = high.shape
    features = back.shape[1]
    units = hidden.shape[1]
    whole = lambda *shape: pl.BlockSpec(shape, lambda i: (0, 0))
    part = lambda rows: pl.BlockSpec((rows, tile), lambda i: (0, i))
    return pl.pallas_call(
        combine_kernel,
        grid=(features // tile,),
        in_specs=[
            whole(count, slots),
            whole(count, slots),
            part(slots),
            whole(count, units),
            part(units),
        ],
        out_specs=part(count),
        out_shape=jax.ShapeDtypeStruct((count, features), dtype),
        cost_estimate=pl.CostEstimate(
            flops=2 * count * features * (2 * slots + units),
            bytes_accessed=4 * count * slots + 2 * slots * features + 4 * count * features,
            transcendentals=0,
        ),
        name="combine",
    )(high, low, back, hidden, down)


def body(
    tokens,
    routes,
    route_weights,
    norm_gain,
    gate_trained,
    up_trained,
    down_trained,
    shared_gate_trained,
    shared_up_trained,
    shared_down_trained,
):
    gr, zl, y = (lax.axis_index(a) for a in ("gr", "zl", "y"))
    n_gr, n_zl, n_y = (lax.axis_size(a) for a in ("gr", "zl", "y"))
    n_xc = lax.axis_size("x") * lax.axis_size("c")
    n_plane = n_y * n_xc
    row_count, features = tokens.shape
    top = routes.shape[1]
    experts, own_hidden, own_cols = gate_trained.shape
    capacity = max(2, 3 * row_count * top // (2 * experts))

    meta = jnp.concatenate([routes.T.astype(f32), route_weights.T], axis=0)
    metas = [meta] + [swapped(meta, "zl", n_zl, k) for k in range(1, n_zl)]
    values = tokens.astype(f32)
    normed = (
        values * lax.rsqrt(jnp.mean(values * values, axis=1, keepdims=True) + epsilon)
    ).astype(bf16)
    blocks = [normed] + [swapped(normed, "zl", n_zl, k) for k in range(1, n_zl)]

    gain = norm_gain[None, :]
    shared = jnp.stack(
        [shared_gate_trained * gain, shared_up_trained * gain, shared_down_trained], axis=0
    ).astype(bf16)
    other = swapped(shared, "gr", n_gr, 1)
    shared = jnp.where(gr == 0, jnp.stack([shared, other]), jnp.stack([other, shared]))

    steps = range(n_gr * n_zl)
    place = jnp.stack([v for k in steps for v in (zl ^ (k % n_zl), gr ^ (k // n_zl))])
    place = place.astype(jnp.int32)
    sent = cast(place, norm_gain[None, :], gate_trained, up_trained, down_trained, n_plane)
    landed = plane_exchange(sent)
    piece = 3 * own_hidden
    moved = [landed[:, j * piece : (j + 1) * piece] for j in range(n_zl)]
    parts = [moved[0]] + [swapped(moved[k % n_zl], ("gr", "zl"), n_gr * n_zl, k) for k in steps[1:]]

    first = zl * n_plane
    near_picks = selection(metas[:2], first, n_plane, top, capacity)
    far_picks = selection(metas[2:], first, n_plane, top, capacity)

    def dispatched(code, rows, after):
        out = pick(code, *rows, 2 * capacity, 256)
        out, _ = lax.optimization_barrier((out, after))
        return plane_exchange(out.reshape(n_plane, 2 * capacity, features))

    near_in = dispatched(near_picks[0], blocks[:2], landed)
    far_in = dispatched(far_picks[0], blocks[2:], near_in)

    share = shared.shape[2]
    extra = jnp.broadcast_to(
        shared.reshape(1, -1, own_cols), (n_plane, shared.size // own_cols, own_cols)
    )
    extra, _ = lax.optimization_barrier((extra, far_in))
    quarter = plane_exchange(extra).reshape(n_y, n_xc, n_gr, 3, share, own_cols)
    quarter = quarter.transpose(3, 0, 4, 2, 1, 5).reshape(3, n_y * share, features)
    shared_out = [
        lax.dynamic_slice_in_dim(quarter[m], y * share, share, axis=0) for m in range(3)
    ]

    def shared_hidden(pair):
        contract = (((1,), (1,)), ((), ()))
        done = []
        for rows in pair:
            g = lax.dot_general(rows, quarter[0], contract, preferred_element_type=f32)
            u = lax.dot_general(rows, quarter[1], contract, preferred_element_type=f32)
            done.append((jax.nn.silu(g) * u).astype(bf16))
        return jnp.concatenate(done, axis=0)

    near_hidden = shared_hidden(blocks[:2])
    far_hidden = shared_hidden(blocks[2:])
    shared_down = quarter[2]
    far_in, near_hidden, far_hidden, shared_down = lax.optimization_barrier(
        (far_in, near_hidden, far_hidden, shared_down)
    )

    far_result, expert_gate, expert_up, expert_down = ffn_assemble(
        place, far_in.reshape(-1, features), parts, n_y, n_xc, own_hidden, 256
    )
    far_back = plane_exchange(far_result.reshape(n_plane, 2 * capacity, features))
    near_result = ffn(near_in.reshape(-1, features), expert_gate, expert_up, expert_down, 256)
    near_back = plane_exchange(near_result.reshape(n_plane, 2 * capacity, features))

    far_sum = combine(
        *far_picks[1:], far_back.reshape(-1, features), far_hidden, shared_down, bf16, 512
    )
    third = swapped(far_sum[:row_count], "zl", n_zl, 2)
    fourth = swapped(far_sum[row_count:], "zl", n_zl, 3)
    near_sum = combine(
        *near_picks[1:], near_back.reshape(-1, features), near_hidden, shared_down, f32, 512
    )
    second = swapped(near_sum[row_count:].astype(bf16), "zl", n_zl, 1)
    combined = (
        near_sum[:row_count] + second.astype(f32) + third.astype(f32) + fourth.astype(f32)
    ).astype(bf16)
    return (combined, expert_gate, expert_up, expert_down, *shared_out)


def solution(mesh):
    fine = Mesh(mesh.devices.reshape(2, 4, 4, 4, 2), ALL)
    cols = ("gr", "x", "c")
    in_specs = (
        P(ALL, None),
        P(ALL, None),
        P(ALL, None),
        P(cols),
        P(None, ("zl", "y"), cols),
        P(None, ("zl", "y"), cols),
        P(None, ("zl", "y"), cols),
        P(("zl", "y"), cols),
        P(("zl", "y"), cols),
        P(("zl", "y"), cols),
    )
    out_specs = (
        P(ALL, None),
        P(("zl", "y", "x", "c"), None, None),
        P(("zl", "y", "x", "c"), None, None),
        P(("zl", "y", "x", "c"), None, None),
        P(("zl", "y"), None),
        P(("zl", "y"), None),
        P(("zl", "y"), None),
    )

    def step(*args):
        return body(*args)

    step = jax.shard_map(step, mesh=fine, in_specs=in_specs, out_specs=out_specs, check_vma=False)
    return step
```

```python
import functools

import jax
import jax.numpy as jnp
from jax import lax
from jax.experimental import pallas as pl
from jax.experimental.pallas import tpu as pltpu
from jax.sharding import Mesh, PartitionSpec as P


epsilon = 1e-06
ALL = ("gr", "zl", "y", "x", "c")
PLANE = ("y", "x", "c")
bf16 = jnp.bfloat16
f32 = jnp.float32


def swapped(array, axis, size, k):
    return lax.ppermute(array, axis, [(r, r ^ k) for r in range(size)])


def plane_exchange(array):
    return lax.all_to_all(array, PLANE, split_axis=0, concat_axis=0, tiled=True)


def ffn_rows(x, gate, up, down):
    contract = (((1,), (1,)), ((), ()))
    g = lax.dot_general(x, gate, contract, preferred_element_type=f32)
    u = lax.dot_general(x, up, contract, preferred_element_type=f32)
    hidden = (jax.nn.silu(g) * u).astype(bf16)
    return jnp.dot(hidden, down, preferred_element_type=f32)


def cast_kernel(place, gain, gate, up, down, out):
    n = gate.shape[1]
    scale = gain[...][None]
    out[:, :n, :] = (gate[...] * scale).astype(bf16)
    out[:, n : 2 * n, :] = (up[...] * scale).astype(bf16)
    out[:, 2 * n :, :] = down[...].astype(bf16)


def cast(place, gain, gate, up, down, n_plane):
    experts, n, cols = gate.shape
    n_zl = experts // n_plane
    piece = pl.BlockSpec((n_plane, n, cols), lambda j, p: (p[0] ^ j, 0, 0))
    spec = pltpu.PrefetchScalarGridSpec(
        num_scalar_prefetch=1,
        grid=(n_zl,),
        in_specs=[pl.BlockSpec((1, cols), lambda j, p: (0, 0)), piece, piece, piece],
        out_specs=pl.BlockSpec((n_plane, 3 * n, cols), lambda j, p: (0, j, 0)),
    )
    return pl.pallas_call(
        cast_kernel,
        grid_spec=spec,
        out_shape=jax.ShapeDtypeStruct((n_plane, n_zl * 3 * n, cols), bf16),
        cost_estimate=pl.CostEstimate(
            flops=3 * gate.size, bytes_accessed=18 * gate.size, transcendentals=0
        ),
        name="cast",
    )(place, gain, gate, up, down)


def ffn_assemble_kernel(place, x, *refs, blocks, n_y, n_xc, own_hidden, cols):
    parts, refs = refs[:blocks], refs[blocks:]
    out, outs, held, sems = refs[0], refs[1:4], refs[4:7], refs[7]
    step = pl.program_id(0)
    n_cols = held[0].shape[0]

    def writes():
        return [
            pltpu.make_async_copy(
                held[m].at[f],
                outs[m].at[0, :, pl.ds(f * cols, cols)],
                sems.at[blocks * 3 * n_y + m * n_cols + f],
            )
            for m in range(3)
            for f in range(n_cols)
        ]

    @pl.when(step == 0)
    def _():
        reads = []
        for k in range(blocks):
            row = place[2 * k] * (n_y * own_hidden)
            col = place[2 * k + 1] * n_xc
            for m in range(3):
                for y in range(n_y):
                    at = pl.multiple_of(row + y * own_hidden, 8)
                    reads.append(
                        pltpu.make_async_copy(
                            parts[k].at[pl.ds(y * n_xc, n_xc), pl.ds(m * own_hidden, own_hidden)],
                            held[m].at[pl.ds(col, n_xc), pl.ds(at, own_hidden)],
                            sems.at[(k * 3 + m) * n_y + y],
                        )
                    )
        for r in reads:
            r.start()
        for r in reads:
            r.wait()
        for w in writes():
            w.start()

    gate, up, down = (
        jnp.concatenate([held[m][f] for f in range(n_cols)], axis=1) for m in range(3)
    )
    out[...] = ffn_rows(x[...], gate, up, down).astype(bf16)

    @pl.when(step == pl.num_programs(0) - 1)
    def _():
        for w in writes():
            w.wait()


def ffn_assemble(place, x, parts, n_y, n_xc, own_hidden, tile):
    count, features = x.shape
    cols = parts[0].shape[2]
    n_cols = features // cols
    hidden = len(parts) * n_y * n_xc * own_hidden * cols // features
    matrix = jax.ShapeDtypeStruct((1, hidden, features), bf16)
    hbm = pl.BlockSpec(memory_space=pl.ANY)
    spec = pltpu.PrefetchScalarGridSpec(
        num_scalar_prefetch=1,
        grid=(count // tile,),
        in_specs=[pl.BlockSpec((tile, features), lambda i, p: (i, 0))] + [hbm] * len(parts),
        out_specs=[pl.BlockSpec((tile, features), lambda i, p: (i, 0))] + [hbm] * 3,
        scratch_shapes=[pltpu.VMEM((n_cols, hidden, cols), bf16)] * 3
        + [pltpu.SemaphoreType.DMA((len(parts) * 3 * n_y + 3 * n_cols,))],
    )
    return pl.pallas_call(
        functools.partial(
            ffn_assemble_kernel,
            blocks=len(parts),
            n_y=n_y,
            n_xc=n_xc,
            own_hidden=own_hidden,
            cols=cols,
        ),
        grid_spec=spec,
        out_shape=[jax.ShapeDtypeStruct((count, features), bf16)] + [matrix] * 3,
        cost_estimate=pl.CostEstimate(
            flops=6 * count * hidden * features,
            bytes_accessed=4 * count * features + 12 * hidden * features,
            transcendentals=count * hidden,
        ),
        name="ffn_assemble",
    )(place, x, *parts)


def ffn_kernel(x, gate, up, down, out):
    out[...] = ffn_rows(x[...], gate[0], up[0], down[0]).astype(bf16)


def ffn(x, gate, up, down, tile):
    count, features = x.shape
    hidden = gate.shape[1]
    whole = pl.BlockSpec((1, hidden, features), lambda i: (0, 0, 0))
    rows = pl.BlockSpec((tile, features), lambda i: (i, 0))
    return pl.pallas_call(
        ffn_kernel,
        grid=(count // tile,),
        in_specs=[rows, whole, whole, whole],
        out_specs=rows,
        out_shape=jax.ShapeDtypeStruct((count, features), bf16),
        cost_estimate=pl.CostEstimate(
            flops=6 * count * hidden * features,
            bytes_accessed=4 * count * features + 6 * hidden * features,
            transcendentals=count * hidden,
        ),
        name="ffn_rows",
    )(x, gate, up, down)


def selection(metas, first, experts, top, capacity):
    codes, weights = [], []
    for k, meta in enumerate(metas):
        names = meta[:top] - first.astype(f32)
        hits = names[:, None, :] == jnp.arange(experts, dtype=f32)[None, :, None]
        chosen = jnp.sum(hits.astype(f32), axis=0)
        weight = jnp.sum(jnp.where(hits, meta[top:, None, :], 0.0), axis=0)
        n = chosen.shape[1]
        before = (jnp.arange(n)[:, None] < jnp.arange(n)[None, :]).astype(bf16)
        place = jnp.dot(chosen.astype(bf16), before, preferred_element_type=f32)
        codes.append(jnp.where(chosen > 0, place + float(k * capacity), -1.0))
        weights.append(weight)
    code = jnp.concatenate(codes, axis=1).astype(bf16)
    weight = jnp.concatenate(weights, axis=1)
    high = weight.astype(bf16)
    low = (weight - high.astype(f32)).astype(bf16)
    span = len(metas) * capacity
    slot = jnp.arange(experts * span, dtype=jnp.int32)
    within = (slot % span).astype(f32)
    spread = (slot[:, None] // span == jnp.arange(experts, dtype=jnp.int32)[None, :]).astype(bf16)

    def by_token(values):
        return lax.dot_general(
            values, spread, (((0,), (1,)), ((), ())), preferred_element_type=f32
        )

    held = by_token(code) == within[None, :]
    high = jnp.where(held, by_token(high), 0.0).astype(bf16)
    low = jnp.where(held, by_token(low), 0.0).astype(bf16)
    return code, high, low


def pick_kernel(code, one, two, out, *, span, tile):
    slot = lax.broadcasted_iota(jnp.int32, (tile, 1), 0) + pl.program_id(0) * tile
    expert = slot // span
    within = (slot - expert * span).astype(f32)
    names = lax.broadcasted_iota(jnp.int32, (tile, code.shape[0]), 1)
    spread = (names == expert).astype(f32).astype(bf16)
    held = jnp.dot(spread, code[...], preferred_element_type=f32) == within
    held = held.astype(f32).astype(bf16)
    n = one.shape[0]
    total = jnp.dot(held[:, :n], one[...], preferred_element_type=f32)
    total += jnp.dot(held[:, n:], two[...], preferred_element_type=f32)
    out[...] = total.astype(bf16)


def pick(code, one, two, span, tile):
    experts, count = code.shape
    features = one.shape[1]
    slots = experts * span
    whole = lambda a: pl.BlockSpec(a.shape, lambda i: (0, 0))
    return pl.pallas_call(
        functools.partial(pick_kernel, span=span, tile=tile),
        grid=(slots // tile,),
        in_specs=[whole(code), whole(one), whole(two)],
        out_specs=pl.BlockSpec((tile, features), lambda i: (i, 0)),
        out_shape=jax.ShapeDtypeStruct((slots, features), bf16),
        cost_estimate=pl.CostEstimate(
            flops=2 * slots * count * features,
            bytes_accessed=2 * (slots + count) * features,
            transcendentals=0,
        ),
        name="pick",
    )(code, one, two)


def lay_kernel(place, stack, out):
    n, groups, _, _, cols = stack.shape
    for g in range(groups):
        for i in range(n):
            at = (g * n + i) * cols
            out[:, :, at : at + cols] = stack[i ^ place[0], g]


def lay(place, stack):
    n, groups, matrices, rows, cols = stack.shape
    spec = pltpu.PrefetchScalarGridSpec(
        num_scalar_prefetch=1,
        grid=(1,),
        in_specs=[pl.BlockSpec(stack.shape, lambda i, p: (0,) * 5)],
        out_specs=pl.BlockSpec((matrices, rows, groups * n * cols), lambda i, p: (0, 0, 0)),
    )
    return pl.pallas_call(
        lay_kernel,
        grid_spec=spec,
        out_shape=jax.ShapeDtypeStruct((matrices, rows, groups * n * cols), bf16),
        cost_estimate=pl.CostEstimate(
            flops=stack.size, bytes_accessed=4 * stack.size, transcendentals=0
        ),
        name="lay",
    )(place, stack)


def combine_kernel(high, low, back, hidden, down, one, two):
    rows = back[...]
    total = jnp.dot(high[...], rows, preferred_element_type=f32)
    total += jnp.dot(low[...], rows, preferred_element_type=f32)
    total += jnp.dot(hidden[...], down[...], preferred_element_type=f32)
    n = one.shape[0]
    one[...] = total[:n].astype(one.dtype)
    two[...] = total[n:].astype(two.dtype)


def combine(high, low, back, hidden, down, dtypes, tile):
    count, slots = high.shape
    features = back.shape[1]
    units = hidden.shape[1]
    whole = lambda *shape: pl.BlockSpec(shape, lambda i: (0, 0))
    part = lambda rows: pl.BlockSpec((rows, tile), lambda i: (0, i))
    return pl.pallas_call(
        combine_kernel,
        grid=(features // tile,),
        in_specs=[
            whole(count, slots),
            whole(count, slots),
            part(slots),
            whole(count, units),
            part(units),
        ],
        out_specs=[part(count // 2)] * 2,
        out_shape=[jax.ShapeDtypeStruct((count // 2, features), d) for d in dtypes],
        cost_estimate=pl.CostEstimate(
            flops=2 * count * features * (2 * slots + units),
            bytes_accessed=4 * count * slots + 2 * slots * features + 4 * count * features,
            transcendentals=0,
        ),
        name="combine",
    )(high, low, back, hidden, down)


def body(
    tokens,
    routes,
    route_weights,
    norm_gain,
    gate_trained,
    up_trained,
    down_trained,
    shared_gate_trained,
    shared_up_trained,
    shared_down_trained,
):
    gr, zl, _ = (lax.axis_index(a) for a in ("gr", "zl", "y"))
    n_gr, n_zl, n_y = (lax.axis_size(a) for a in ("gr", "zl", "y"))
    n_xc = lax.axis_size("x") * lax.axis_size("c")
    n_plane = n_y * n_xc
    row_count, features = tokens.shape
    top = routes.shape[1]
    experts, own_hidden, _ = gate_trained.shape
    capacity = max(2, 3 * row_count * top // (2 * experts))

    meta = jnp.concatenate([routes.T.astype(f32), route_weights.T], axis=0)
    metas = [meta] + [swapped(meta, "zl", n_zl, k) for k in range(1, n_zl)]
    values = tokens.astype(f32)
    normed = (
        values * lax.rsqrt(jnp.mean(values * values, axis=1, keepdims=True) + epsilon)
    ).astype(bf16)
    blocks = [normed] + [swapped(normed, "zl", n_zl, k) for k in range(1, n_zl)]

    gain = norm_gain[None, :]
    shared = jnp.stack(
        [shared_gate_trained * gain, shared_up_trained * gain, shared_down_trained], axis=0
    ).astype(bf16)
    other = swapped(shared, "gr", n_gr, 1)
    shared = jnp.where(gr == 0, jnp.stack([shared, other]), jnp.stack([other, shared]))

    steps = range(n_gr * n_zl)
    place = jnp.stack([v for k in steps for v in (zl ^ (k % n_zl), gr ^ (k // n_zl))])
    place = place.astype(jnp.int32)
    sent = cast(place, norm_gain[None, :], gate_trained, up_trained, down_trained, n_plane)
    landed = plane_exchange(sent)
    piece = 3 * own_hidden
    moved = [landed[:, j * piece : (j + 1) * piece] for j in range(n_zl)]
    parts = [moved[0]] + [swapped(moved[k % n_zl], ("gr", "zl"), n_gr * n_zl, k) for k in steps[1:]]

    first = zl * n_plane
    near_picks = selection(metas[:2], first, n_plane, top, capacity)
    far_picks = selection(metas[2:], first, n_plane, top, capacity)

    def dispatched(code, rows, after):
        out = pick(code, *rows, 2 * capacity, 256)
        out, _ = lax.optimization_barrier((out, after))
        return plane_exchange(out.reshape(n_plane, 2 * capacity, features))

    near_in = dispatched(near_picks[0], blocks[:2], landed)
    far_in = dispatched(far_picks[0], blocks[2:], near_in)

    laid = [shared] + [swapped(shared, ("x", "c"), n_xc, k) for k in range(1, n_xc)]
    across = (lax.axis_index("x") * lax.axis_size("c") + lax.axis_index("c"))[None]
    own = lay(across.astype(jnp.int32), jnp.stack(laid))
    quarter = jnp.concatenate([own] + [swapped(own, "y", n_y, k) for k in range(1, n_y)], axis=1)
    shared_out = [own[m] for m in range(3)]

    def shared_hidden(pair):
        contract = (((1,), (1,)), ((), ()))
        done = []
        for rows in pair:
            g = lax.dot_general(rows, quarter[0], contract, preferred_element_type=f32)
            u = lax.dot_general(rows, quarter[1], contract, preferred_element_type=f32)
            done.append((jax.nn.silu(g) * u).astype(bf16))
        return jnp.concatenate(done, axis=0)

    near_hidden = shared_hidden(blocks[:2])
    far_hidden = shared_hidden(blocks[2:])
    shared_down = quarter[2]
    far_in, near_hidden, far_hidden, shared_down = lax.optimization_barrier(
        (far_in, near_hidden, far_hidden, shared_down)
    )

    far_result, expert_gate, expert_up, expert_down = ffn_assemble(
        place, far_in.reshape(-1, features), parts, n_y, n_xc, own_hidden, 256
    )
    far_back = plane_exchange(far_result.reshape(n_plane, 2 * capacity, features))
    near_result = ffn(
        near_in.reshape(-1, features), expert_gate, expert_up, expert_down, 256
    )
    near_back = plane_exchange(near_result.reshape(n_plane, 2 * capacity, features))

    third, fourth = combine(
        *far_picks[1:],
        far_back.reshape(-1, features),
        far_hidden,
        shared_down,
        (bf16, bf16),
        512,
    )
    third = swapped(third, "zl", n_zl, 2)
    fourth = swapped(fourth, "zl", n_zl, 3)
    kept, second = combine(
        *near_picks[1:],
        near_back.reshape(-1, features),
        near_hidden,
        shared_down,
        (f32, bf16),
        512,
    )
    second = swapped(second, "zl", n_zl, 1)
    combined = (
        kept + second.astype(f32) + third.astype(f32) + fourth.astype(f32)
    ).astype(bf16)
    return (combined, expert_gate, expert_up, expert_down, *shared_out)


def solution(mesh):
    fine = Mesh(mesh.devices.reshape(2, 4, 4, 4, 2), ALL)
    cols = ("gr", "x", "c")
    in_specs = (
        P(ALL, None),
        P(ALL, None),
        P(ALL, None),
        P(cols),
        P(None, ("zl", "y"), cols),
        P(None, ("zl", "y"), cols),
        P(None, ("zl", "y"), cols),
        P(("zl", "y"), cols),
        P(("zl", "y"), cols),
        P(("zl", "y"), cols),
    )
    out_specs = (
        P(ALL, None),
        P(("zl", "y", "x", "c"), None, None),
        P(("zl", "y", "x", "c"), None, None),
        P(("zl", "y", "x", "c"), None, None),
        P(("zl", "y"), None),
        P(("zl", "y"), None),
        P(("zl", "y"), None),
    )

    def step(*args):
        return body(*args)

    step = jax.shard_map(step, mesh=fine, in_specs=in_specs, out_specs=out_specs, check_vma=False)
    return step
```

```python
import functools

import jax
import jax.numpy as jnp
from jax import lax
from jax.experimental import pallas as pl
from jax.experimental.pallas import tpu as pltpu
from jax.sharding import Mesh, PartitionSpec as P


epsilon = 1e-06
ALL = ("gr", "zl", "y", "x", "c")
PLANE = ("y", "x", "c")
bf16 = jnp.bfloat16
f32 = jnp.float32


def swapped(array, axis, size, k):
    return lax.ppermute(array, axis, [(r, r ^ k) for r in range(size)])


def plane_exchange(array):
    return lax.all_to_all(array, PLANE, split_axis=0, concat_axis=0, tiled=True)


def cast_kernel(place, gain, gate, up, down, out):
    n = gate.shape[1]
    scale = gain[...][None]
    out[:, :n, :] = (gate[...] * scale).astype(bf16)
    out[:, n : 2 * n, :] = (up[...] * scale).astype(bf16)
    out[:, 2 * n :, :] = down[...].astype(bf16)


def cast(place, gain, gate, up, down, n_plane):
    experts, n, cols = gate.shape
    n_zl = experts // n_plane
    piece = pl.BlockSpec((n_plane, n, cols), lambda j, p: (p[0] ^ j, 0, 0))
    spec = pltpu.PrefetchScalarGridSpec(
        num_scalar_prefetch=1,
        grid=(n_zl,),
        in_specs=[pl.BlockSpec((1, cols), lambda j, p: (0, 0)), piece, piece, piece],
        out_specs=pl.BlockSpec((n_plane, 3 * n, cols), lambda j, p: (0, j, 0)),
    )
    return pl.pallas_call(
        cast_kernel,
        grid_spec=spec,
        out_shape=jax.ShapeDtypeStruct((n_plane, n_zl * 3 * n, cols), bf16),
        cost_estimate=pl.CostEstimate(
            flops=3 * gate.size, bytes_accessed=18 * gate.size, transcendentals=0
        ),
        name="cast",
    )(place, gain, gate, up, down)


def hidden_rows(x, gate, up):
    contract = (((1,), (1,)), ((), ()))
    g = lax.dot_general(x, gate, contract, preferred_element_type=f32)
    u = lax.dot_general(x, up, contract, preferred_element_type=f32)
    return (jax.nn.silu(g) * u).astype(bf16)


def down_rows(hidden, down):
    return jnp.dot(hidden, down, preferred_element_type=f32).astype(bf16)


def assemble_kernel(place, x, *refs, compute, blocks, matrices, n_y, n_xc, own_hidden, cols):
    parts, refs = refs[:blocks], refs[blocks:]
    out, outs, held, sems = refs[0], refs[1 : 1 + matrices], refs[1 + matrices : -1], refs[-1]
    step = pl.program_id(0)
    n_cols = held[0].shape[0]

    def writes():
        return [
            pltpu.make_async_copy(
                held[m].at[f],
                outs[m].at[0, :, pl.ds(f * cols, cols)],
                sems.at[blocks * matrices * n_y + m * n_cols + f],
            )
            for m in range(matrices)
            for f in range(n_cols)
        ]

    @pl.when(step == 0)
    def _():
        reads = []
        for k in range(blocks):
            row = place[2 * k] * (n_y * own_hidden)
            col = place[2 * k + 1] * n_xc
            for m in range(matrices):
                for y in range(n_y):
                    at = pl.multiple_of(row + y * own_hidden, 8)
                    reads.append(
                        pltpu.make_async_copy(
                            parts[k].at[pl.ds(y * n_xc, n_xc), pl.ds(m * own_hidden, own_hidden)],
                            held[m].at[pl.ds(col, n_xc), pl.ds(at, own_hidden)],
                            sems.at[(k * matrices + m) * n_y + y],
                        )
                    )
        for r in reads:
            r.start()
        for r in reads:
            r.wait()
        for w in writes():
            w.start()

    whole = [jnp.concatenate([h[f] for f in range(n_cols)], axis=1) for h in held]
    out[...] = compute(x[...], *whole)

    @pl.when(step == pl.num_programs(0) - 1)
    def _():
        for w in writes():
            w.wait()


def assemble(compute, place, x, parts, matrices, features, width, n_y, n_xc, own_hidden, tile):
    count, depth = x.shape
    cols = parts[0].shape[2]
    n_cols = features // cols
    hidden = len(parts) * n_y * n_xc * own_hidden * cols // features
    matrix = jax.ShapeDtypeStruct((1, hidden, features), bf16)
    hbm = pl.BlockSpec(memory_space=pl.ANY)
    spec = pltpu.PrefetchScalarGridSpec(
        num_scalar_prefetch=1,
        grid=(count // tile,),
        in_specs=[pl.BlockSpec((tile, depth), lambda i, p: (i, 0))] + [hbm] * len(parts),
        out_specs=[pl.BlockSpec((tile, width), lambda i, p: (i, 0))] + [hbm] * matrices,
        scratch_shapes=[pltpu.VMEM((n_cols, hidden, cols), bf16)] * matrices
        + [pltpu.SemaphoreType.DMA((len(parts) * matrices * n_y + matrices * n_cols,))],
    )
    return pl.pallas_call(
        functools.partial(
            assemble_kernel,
            compute=compute,
            blocks=len(parts),
            matrices=matrices,
            n_y=n_y,
            n_xc=n_xc,
            own_hidden=own_hidden,
            cols=cols,
        ),
        grid_spec=spec,
        out_shape=[jax.ShapeDtypeStruct((count, width), bf16)] + [matrix] * matrices,
        cost_estimate=pl.CostEstimate(
            flops=2 * matrices * count * hidden * features,
            bytes_accessed=4 * count * features + 4 * matrices * hidden * features,
            transcendentals=count * hidden,
        ),
        name="assemble",
    )(place, x, *parts)


def rows_kernel(x, *refs, compute):
    refs[-1][...] = compute(x[...], *(r[0] for r in refs[:-1]))


def over_rows(compute, x, matrices, width, tile):
    count, depth = x.shape
    whole = pl.BlockSpec(matrices[0].shape, lambda i: (0, 0, 0))
    return pl.pallas_call(
        functools.partial(rows_kernel, compute=compute),
        grid=(count // tile,),
        in_specs=[pl.BlockSpec((tile, depth), lambda i: (i, 0))] + [whole] * len(matrices),
        out_specs=pl.BlockSpec((tile, width), lambda i: (i, 0)),
        out_shape=jax.ShapeDtypeStruct((count, width), bf16),
        cost_estimate=pl.CostEstimate(
            flops=2 * count * sum(m.size for m in matrices),
            bytes_accessed=2 * count * (depth + width) + 2 * sum(m.size for m in matrices),
            transcendentals=count,
        ),
        name="over_rows",
    )(x, *matrices)


def selection(metas, first, experts, top, capacity):
    span = len(metas) * capacity
    slot = jnp.arange(experts * span, dtype=jnp.int32)
    within = (slot % span).astype(f32)
    spread = (slot[:, None] // span == jnp.arange(experts, dtype=jnp.int32)[None, :]).astype(bf16)

    def by_token(values):
        return lax.dot_general(
            values, spread, (((0,), (1,)), ((), ())), preferred_element_type=f32
        )

    codes, weights = [], []
    for k, meta in enumerate(metas):
        names = meta[:top] - first.astype(f32)
        hits = names[:, None, :] == jnp.arange(experts, dtype=f32)[None, :, None]
        chosen = jnp.sum(hits.astype(f32), axis=0)
        weight = jnp.sum(jnp.where(hits, meta[top:, None, :], 0.0), axis=0)
        n = chosen.shape[1]
        before = (jnp.arange(n)[:, None] < jnp.arange(n)[None, :]).astype(bf16)
        place = jnp.dot(chosen.astype(bf16), before, preferred_element_type=f32)
        code = jnp.where(chosen > 0, place + float(k * capacity), -1.0).astype(bf16)
        high = weight.astype(bf16)
        low = (weight - high.astype(f32)).astype(bf16)
        held = by_token(code) == within[None, :]
        high = jnp.where(held, by_token(high), 0.0).astype(bf16)
        low = jnp.where(held, by_token(low), 0.0).astype(bf16)
        codes.append(code)
        weights.append((high, low))
    return jnp.concatenate(codes, axis=1), weights


def pick_kernel(code, one, two, out, *, span, tile):
    slot = lax.broadcasted_iota(jnp.int32, (tile, 1), 0) + pl.program_id(0) * tile
    expert = slot // span
    within = (slot - expert * span).astype(f32)
    names = lax.broadcasted_iota(jnp.int32, (tile, code.shape[0]), 1)
    spread = (names == expert).astype(f32).astype(bf16)
    held = jnp.dot(spread, code[...], preferred_element_type=f32) == within
    held = held.astype(f32).astype(bf16)
    n = one.shape[0]
    total = jnp.dot(held[:, :n], one[...], preferred_element_type=f32)
    total += jnp.dot(held[:, n:], two[...], preferred_element_type=f32)
    out[...] = total.astype(bf16)


def pick(code, one, two, span, tile):
    experts, count = code.shape
    features = one.shape[1]
    slots = experts * span
    whole = lambda a: pl.BlockSpec(a.shape, lambda i: (0, 0))
    return pl.pallas_call(
        functools.partial(pick_kernel, span=span, tile=tile),
        grid=(slots // tile,),
        in_specs=[whole(code), whole(one), whole(two)],
        out_specs=pl.BlockSpec((tile, features), lambda i: (i, 0)),
        out_shape=jax.ShapeDtypeStruct((slots, features), bf16),
        cost_estimate=pl.CostEstimate(
            flops=2 * slots * count * features,
            bytes_accessed=2 * (slots + count) * features,
            transcendentals=0,
        ),
        name="pick",
    )(code, one, two)


def lay_kernel(place, stack, out):
    n, groups, _, _, cols = stack.shape
    for g in range(groups):
        for i in range(n):
            at = (g * n + i) * cols
            out[:, :, at : at + cols] = stack[i ^ place[0], g]


def lay(place, stack):
    n, groups, matrices, rows, cols = stack.shape
    spec = pltpu.PrefetchScalarGridSpec(
        num_scalar_prefetch=1,
        grid=(1,),
        in_specs=[pl.BlockSpec(stack.shape, lambda i, p: (0,) * 5)],
        out_specs=pl.BlockSpec((matrices, rows, groups * n * cols), lambda i, p: (0, 0, 0)),
    )
    return pl.pallas_call(
        lay_kernel,
        grid_spec=spec,
        out_shape=jax.ShapeDtypeStruct((matrices, rows, groups * n * cols), bf16),
        cost_estimate=pl.CostEstimate(
            flops=stack.size, bytes_accessed=4 * stack.size, transcendentals=0
        ),
        name="lay",
    )(place, stack)


def combine_kernel(high, low, back, hidden, down, out):
    rows = back[...]
    total = jnp.dot(high[...], rows, preferred_element_type=f32)
    total += jnp.dot(low[...], rows, preferred_element_type=f32)
    total += jnp.dot(hidden[...], down[...], preferred_element_type=f32)
    out[...] = total.astype(out.dtype)


def combine(weights, back, hidden, down, dtype, tile):
    high, low = weights
    count, slots = high.shape
    features = back.shape[1]
    units = hidden.shape[1]
    whole = lambda *shape: pl.BlockSpec(shape, lambda i: (0, 0))
    part = lambda rows: pl.BlockSpec((rows, tile), lambda i: (0, i))
    return pl.pallas_call(
        combine_kernel,
        grid=(features // tile,),
        in_specs=[
            whole(count, slots),
            whole(count, slots),
            part(slots),
            whole(count, units),
            part(units),
        ],
        out_specs=part(count),
        out_shape=jax.ShapeDtypeStruct((count, features), dtype),
        cost_estimate=pl.CostEstimate(
            flops=2 * count * features * (2 * slots + units),
            bytes_accessed=4 * count * slots + 2 * slots * features + 4 * count * features,
            transcendentals=0,
        ),
        name="combine",
    )(high, low, back, hidden, down)


def body(
    tokens,
    routes,
    route_weights,
    norm_gain,
    gate_trained,
    up_trained,
    down_trained,
    shared_gate_trained,
    shared_up_trained,
    shared_down_trained,
):
    gr, zl, _ = (lax.axis_index(a) for a in ("gr", "zl", "y"))
    n_gr, n_zl, n_y = (lax.axis_size(a) for a in ("gr", "zl", "y"))
    n_xc = lax.axis_size("x") * lax.axis_size("c")
    n_plane = n_y * n_xc
    row_count, features = tokens.shape
    top = routes.shape[1]
    experts, own_hidden, _ = gate_trained.shape
    capacity = max(2, 3 * row_count * top // (2 * experts))

    meta = jnp.concatenate([routes.T.astype(f32), route_weights.T], axis=0)
    metas = [meta] + [swapped(meta, "zl", n_zl, k) for k in range(1, n_zl)]
    values = tokens.astype(f32)
    normed = (
        values * lax.rsqrt(jnp.mean(values * values, axis=1, keepdims=True) + epsilon)
    ).astype(bf16)
    blocks = [normed] + [swapped(normed, "zl", n_zl, k) for k in range(1, n_zl)]

    gain = norm_gain[None, :]
    shared = jnp.stack(
        [shared_gate_trained * gain, shared_up_trained * gain, shared_down_trained], axis=0
    ).astype(bf16)
    other = swapped(shared, "gr", n_gr, 1)
    shared = jnp.where(gr == 0, jnp.stack([shared, other]), jnp.stack([other, shared]))

    steps = range(n_gr * n_zl)
    place = jnp.stack([v for k in steps for v in (zl ^ (k % n_zl), gr ^ (k // n_zl))])
    place = place.astype(jnp.int32)
    sent = cast(place, norm_gain[None, :], gate_trained, up_trained, down_trained, n_plane)
    landed = plane_exchange(sent)
    piece = 3 * own_hidden

    def spread(begin, end):
        moved = [landed[:, j * piece + begin : j * piece + end] for j in range(n_zl)]
        return [moved[0]] + [
            swapped(moved[k % n_zl], ("gr", "zl"), n_gr * n_zl, k) for k in steps[1:]
        ]

    first_parts = spread(0, 2 * own_hidden)
    down_parts = spread(2 * own_hidden, piece)

    first = zl * n_plane
    near_picks = selection(metas[:2], first, n_plane, top, capacity)
    far_picks = selection(metas[2:], first, n_plane, top, capacity)

    def dispatched(code, rows, after):
        out = pick(code, *rows, 2 * capacity, 256)
        out, _ = lax.optimization_barrier((out, after))
        return plane_exchange(out.reshape(n_plane, 2 * capacity, features))

    near_in = dispatched(near_picks[0], blocks[:2], landed)
    far_in = dispatched(far_picks[0], blocks[2:], near_in)

    laid = [shared] + [swapped(shared, ("x", "c"), n_xc, k) for k in range(1, n_xc)]
    across = (lax.axis_index("x") * lax.axis_size("c") + lax.axis_index("c"))[None]
    own = lay(across.astype(jnp.int32), jnp.stack(laid))
    columns = [own] + [swapped(own, "y", n_y, k) for k in range(1, n_y)]
    shared_out = [own[m] for m in range(3)]

    hidden = own_hidden * n_zl * n_y
    sizes = (features, hidden, n_y, n_xc, own_hidden, 256)
    near_units, expert_gate, expert_up = assemble(
        hidden_rows, place, near_in.reshape(-1, features), first_parts, 2, *sizes
    )
    far_units = over_rows(
        hidden_rows, far_in.reshape(-1, features), (expert_gate, expert_up), hidden, 256
    )
    far_units, near_weights, far_weights = lax.optimization_barrier(
        (far_units, near_picks[1], far_picks[1])
    )
    sizes = (features, features, n_y, n_xc, own_hidden, 256)
    far_result, expert_down = assemble(down_rows, place, far_units, down_parts, 1, *sizes)
    far_back = plane_exchange(far_result.reshape(n_plane, 2 * capacity, features))
    near_result = over_rows(down_rows, near_units, (expert_down,), features, 256)
    near_back = plane_exchange(near_result.reshape(n_plane, 2 * capacity, features))

    columns, _ = lax.optimization_barrier((columns, far_result))
    quarter = jnp.concatenate(columns, axis=1)
    units = [hidden_rows(rows, quarter[0], quarter[1]) for rows in blocks]
    far_back = far_back.reshape(-1, features)
    near_back = near_back.reshape(-1, features)

    third, fourth = (
        swapped(
            combine(far_weights[k - 2], far_back, units[k], quarter[2], bf16, 512), "zl", n_zl, k
        )
        for k in (2, 3)
    )
    second = swapped(
        combine(near_weights[1], near_back, units[1], quarter[2], bf16, 512), "zl", n_zl, 1
    )
    kept = combine(near_weights[0], near_back, units[0], quarter[2], f32, 512)
    combined = (
        kept + second.astype(f32) + third.astype(f32) + fourth.astype(f32)
    ).astype(bf16)
    return (combined, expert_gate, expert_up, expert_down, *shared_out)


def solution(mesh):
    fine = Mesh(mesh.devices.reshape(2, 4, 4, 4, 2), ALL)
    cols = ("gr", "x", "c")
    in_specs = (
        P(ALL, None),
        P(ALL, None),
        P(ALL, None),
        P(cols),
        P(None, ("zl", "y"), cols),
        P(None, ("zl", "y"), cols),
        P(None, ("zl", "y"), cols),
        P(("zl", "y"), cols),
        P(("zl", "y"), cols),
        P(("zl", "y"), cols),
    )
    out_specs = (
        P(ALL, None),
        P(("zl", "y", "x", "c"), None, None),
        P(("zl", "y", "x", "c"), None, None),
        P(("zl", "y", "x", "c"), None, None),
        P(("zl", "y"), None),
        P(("zl", "y"), None),
        P(("zl", "y"), None),
    )

    def step(*args):
        return body(*args)

    step = jax.shard_map(step, mesh=fine, in_specs=in_specs, out_specs=out_specs, check_vma=False)
    return step
```

```python
import functools

import jax
import jax.numpy as jnp
from jax import lax
from jax.experimental import pallas as pl
from jax.experimental.pallas import tpu as pltpu
from jax.sharding import Mesh, PartitionSpec as P


epsilon = 1e-06
ALL = ("gr", "zl", "y", "x", "c")
PLANE = ("y", "x", "c")
bf16 = jnp.bfloat16
f32 = jnp.float32


def swapped(array, axis, size, k):
    return lax.ppermute(array, axis, [(r, r ^ k) for r in range(size)])


def plane_exchange(array):
    return lax.all_to_all(array, PLANE, split_axis=0, concat_axis=0, tiled=True)


def cast_kernel(place, gain, gate, up, down, out):
    n = gate.shape[1]
    scale = gain[...][None]
    out[:, :n, :] = (gate[...] * scale).astype(bf16)
    out[:, n : 2 * n, :] = (up[...] * scale).astype(bf16)
    out[:, 2 * n :, :] = down[...].astype(bf16)


def cast(place, gain, gate, up, down, n_plane):
    experts, n, cols = gate.shape
    n_zl = experts // n_plane
    piece = pl.BlockSpec((n_plane, n, cols), lambda j, p: (p[0] ^ j, 0, 0))
    spec = pltpu.PrefetchScalarGridSpec(
        num_scalar_prefetch=1,
        grid=(n_zl,),
        in_specs=[pl.BlockSpec((1, cols), lambda j, p: (0, 0)), piece, piece, piece],
        out_specs=pl.BlockSpec((n_plane, 3 * n, cols), lambda j, p: (0, j, 0)),
    )
    return pl.pallas_call(
        cast_kernel,
        grid_spec=spec,
        out_shape=jax.ShapeDtypeStruct((n_plane, n_zl * 3 * n, cols), bf16),
        cost_estimate=pl.CostEstimate(
            flops=3 * gate.size, bytes_accessed=18 * gate.size, transcendentals=0
        ),
        name="cast",
    )(place, gain, gate, up, down)


def hidden_rows(x, gate, up):
    contract = (((1,), (1,)), ((), ()))
    g = lax.dot_general(x, gate, contract, preferred_element_type=f32)
    u = lax.dot_general(x, up, contract, preferred_element_type=f32)
    return (jax.nn.silu(g) * u).astype(bf16)


def down_rows(hidden, down):
    return jnp.dot(hidden, down, preferred_element_type=f32).astype(bf16)


def assemble_kernel(place, x, *refs, compute, blocks, matrices, n_y, n_xc, own_hidden, cols):
    parts, refs = refs[:blocks], refs[blocks:]
    out, outs, held, sems = refs[0], refs[1 : 1 + matrices], refs[1 + matrices : -1], refs[-1]
    step = pl.program_id(0)
    n_cols = held[0].shape[0]

    def writes():
        return [
            pltpu.make_async_copy(
                held[m].at[f],
                outs[m].at[0, :, pl.ds(f * cols, cols)],
                sems.at[blocks * matrices * n_y + m * n_cols + f],
            )
            for m in range(matrices)
            for f in range(n_cols)
        ]

    @pl.when(step == 0)
    def _():
        reads = []
        for k in range(blocks):
            row = place[2 * k] * (n_y * own_hidden)
            col = place[2 * k + 1] * n_xc
            for m in range(matrices):
                for y in range(n_y):
                    at = pl.multiple_of(row + y * own_hidden, 8)
                    reads.append(
                        pltpu.make_async_copy(
                            parts[k].at[pl.ds(y * n_xc, n_xc), pl.ds(m * own_hidden, own_hidden)],
                            held[m].at[pl.ds(col, n_xc), pl.ds(at, own_hidden)],
                            sems.at[(k * matrices + m) * n_y + y],
                        )
                    )
        for r in reads:
            r.start()
        for r in reads:
            r.wait()
        for w in writes():
            w.start()

    whole = [jnp.concatenate([h[f] for f in range(n_cols)], axis=1) for h in held]
    out[...] = compute(x[...], *whole)

    @pl.when(step == pl.num_programs(0) - 1)
    def _():
        for w in writes():
            w.wait()


def assemble(compute, place, x, parts, matrices, features, width, n_y, n_xc, own_hidden, tile):
    count, depth = x.shape
    cols = parts[0].shape[2]
    n_cols = features // cols
    hidden = len(parts) * n_y * n_xc * own_hidden * cols // features
    matrix = jax.ShapeDtypeStruct((1, hidden, features), bf16)
    hbm = pl.BlockSpec(memory_space=pl.ANY)
    spec = pltpu.PrefetchScalarGridSpec(
        num_scalar_prefetch=1,
        grid=(count // tile,),
        in_specs=[pl.BlockSpec((tile, depth), lambda i, p: (i, 0))] + [hbm] * len(parts),
        out_specs=[pl.BlockSpec((tile, width), lambda i, p: (i, 0))] + [hbm] * matrices,
        scratch_shapes=[pltpu.VMEM((n_cols, hidden, cols), bf16)] * matrices
        + [pltpu.SemaphoreType.DMA((len(parts) * matrices * n_y + matrices * n_cols,))],
    )
    return pl.pallas_call(
        functools.partial(
            assemble_kernel,
            compute=compute,
            blocks=len(parts),
            matrices=matrices,
            n_y=n_y,
            n_xc=n_xc,
            own_hidden=own_hidden,
            cols=cols,
        ),
        grid_spec=spec,
        out_shape=[jax.ShapeDtypeStruct((count, width), bf16)] + [matrix] * matrices,
        cost_estimate=pl.CostEstimate(
            flops=2 * matrices * count * hidden * features,
            bytes_accessed=4 * count * features + 4 * matrices * hidden * features,
            transcendentals=count * hidden,
        ),
        name="assemble",
    )(place, x, *parts)


def rows_kernel(x, *refs, compute):
    refs[-1][...] = compute(x[...], *(r[0] for r in refs[:-1]))


def over_rows(compute, x, matrices, width, tile):
    count, depth = x.shape
    whole = pl.BlockSpec(matrices[0].shape, lambda i: (0, 0, 0))
    return pl.pallas_call(
        functools.partial(rows_kernel, compute=compute),
        grid=(count // tile,),
        in_specs=[pl.BlockSpec((tile, depth), lambda i: (i, 0))] + [whole] * len(matrices),
        out_specs=pl.BlockSpec((tile, width), lambda i: (i, 0)),
        out_shape=jax.ShapeDtypeStruct((count, width), bf16),
        cost_estimate=pl.CostEstimate(
            flops=2 * count * sum(m.size for m in matrices),
            bytes_accessed=2 * count * (depth + width) + 2 * sum(m.size for m in matrices),
            transcendentals=count,
        ),
        name="over_rows",
    )(x, *matrices)


def selection(metas, first, experts, top, capacity):
    span = len(metas) * capacity
    slot = jnp.arange(experts * span, dtype=jnp.int32)
    within = (slot % span).astype(f32)
    spread = (slot[:, None] // span == jnp.arange(experts, dtype=jnp.int32)[None, :]).astype(bf16)

    def by_token(values):
        return lax.dot_general(
            values, spread, (((0,), (1,)), ((), ())), preferred_element_type=f32
        )

    codes, weights = [], []
    for k, meta in enumerate(metas):
        names = meta[:top] - first.astype(f32)
        hits = names[:, None, :] == jnp.arange(experts, dtype=f32)[None, :, None]
        chosen = jnp.sum(hits.astype(f32), axis=0)
        weight = jnp.sum(jnp.where(hits, meta[top:, None, :], 0.0), axis=0)
        n = chosen.shape[1]
        before = (jnp.arange(n)[:, None] < jnp.arange(n)[None, :]).astype(bf16)
        place = jnp.dot(chosen.astype(bf16), before, preferred_element_type=f32)
        codes.append(jnp.where(chosen > 0, place + float(k * capacity), -1.0))
        weights.append(weight)
    code = jnp.concatenate(codes, axis=1).astype(bf16)
    weight = jnp.concatenate(weights, axis=1)
    high = weight.astype(bf16)
    low = (weight - high.astype(f32)).astype(bf16)
    held = by_token(code) == within[None, :]
    high = jnp.where(held, by_token(high), 0.0).astype(bf16)
    low = jnp.where(held, by_token(low), 0.0).astype(bf16)
    return code, (high, low)


def pick_kernel(code, one, two, out, *, span, tile):
    slot = lax.broadcasted_iota(jnp.int32, (tile, 1), 0) + pl.program_id(0) * tile
    expert = slot // span
    within = (slot - expert * span).astype(f32)
    names = lax.broadcasted_iota(jnp.int32, (tile, code.shape[0]), 1)
    spread = (names == expert).astype(f32).astype(bf16)
    held = jnp.dot(spread, code[...], preferred_element_type=f32) == within
    held = held.astype(f32).astype(bf16)
    n = one.shape[0]
    total = jnp.dot(held[:, :n], one[...], preferred_element_type=f32)
    total += jnp.dot(held[:, n:], two[...], preferred_element_type=f32)
    out[...] = total.astype(bf16)


def pick(code, one, two, span, tile):
    experts, count = code.shape
    features = one.shape[1]
    slots = experts * span
    whole = lambda a: pl.BlockSpec(a.shape, lambda i: (0, 0))
    return pl.pallas_call(
        functools.partial(pick_kernel, span=span, tile=tile),
        grid=(slots // tile,),
        in_specs=[whole(code), whole(one), whole(two)],
        out_specs=pl.BlockSpec((tile, features), lambda i: (i, 0)),
        out_shape=jax.ShapeDtypeStruct((slots, features), bf16),
        cost_estimate=pl.CostEstimate(
            flops=2 * slots * count * features,
            bytes_accessed=2 * (slots + count) * features,
            transcendentals=0,
        ),
        name="pick",
    )(code, one, two)


def lay_kernel(place, *refs):
    pieces, out, held = refs[:-2], refs[-2], refs[-1]
    n = len(pieces)
    groups, _, _, cols = pieces[0].shape
    for k in range(n):
        for g in range(groups):
            held[g * n + (k ^ place[0])] = pieces[k][g]
    for f in range(groups * n):
        out[:, :, f * cols : (f + 1) * cols] = held[f]


def lay(place, pieces):
    n = len(pieces)
    groups, matrices, rows, cols = pieces[0].shape
    piece = pl.BlockSpec(pieces[0].shape, lambda i, p: (0,) * 4)
    spec = pltpu.PrefetchScalarGridSpec(
        num_scalar_prefetch=1,
        grid=(1,),
        in_specs=[piece] * n,
        out_specs=pl.BlockSpec((matrices, rows, groups * n * cols), lambda i, p: (0, 0, 0)),
        scratch_shapes=[pltpu.VMEM((groups * n, matrices, rows, cols), bf16)],
    )
    return pl.pallas_call(
        lay_kernel,
        grid_spec=spec,
        out_shape=jax.ShapeDtypeStruct((matrices, rows, groups * n * cols), bf16),
        cost_estimate=pl.CostEstimate(
            flops=n * pieces[0].size, bytes_accessed=4 * n * pieces[0].size, transcendentals=0
        ),
        name="lay",
    )(place, *pieces)


def units_kernel(*refs, blocks):
    tokens, refs = refs[:blocks], refs[blocks:]
    columns, (near, far, down) = refs[:-3], refs[-3:]
    gate, up, last = (jnp.concatenate([c[m] for c in columns], axis=0) for m in range(3))
    down[...] = last
    half = blocks // 2
    for out, pair in ((near, tokens[:half]), (far, tokens[half:])):
        rows = jnp.concatenate([t[...] for t in pair], axis=0)
        out[...] = hidden_rows(rows, gate, up)


def shared_units(tokens, columns):
    count, features = tokens[0].shape
    units = len(columns) * columns[0].shape[1]
    half = len(tokens) // 2 * count
    return pl.pallas_call(
        functools.partial(units_kernel, blocks=len(tokens)),
        out_shape=[jax.ShapeDtypeStruct((half, units), bf16)] * 2
        + [jax.ShapeDtypeStruct((units, features), bf16)],
        cost_estimate=pl.CostEstimate(
            flops=8 * half * units * features,
            bytes_accessed=4 * half * features + 8 * units * features,
            transcendentals=2 * half * units,
        ),
        name="shared_units",
    )(*tokens, *columns)


def combine_kernel(high, low, back, hidden, down, one, two):
    rows = back[...]
    total = jnp.dot(high[...], rows, preferred_element_type=f32)
    total += jnp.dot(low[...], rows, preferred_element_type=f32)
    total += jnp.dot(hidden[...], down[...], preferred_element_type=f32)
    n = one.shape[0]
    one[...] = total[:n].astype(one.dtype)
    two[...] = total[n:].astype(two.dtype)


def combine(weights, back, hidden, down, dtypes, tile):
    high, low = weights
    count, slots = high.shape
    features = back.shape[1]
    units = hidden.shape[1]
    whole = lambda *shape: pl.BlockSpec(shape, lambda i: (0, 0))
    part = lambda rows: pl.BlockSpec((rows, tile), lambda i: (0, i))
    return pl.pallas_call(
        combine_kernel,
        grid=(features // tile,),
        in_specs=[
            whole(count, slots),
            whole(count, slots),
            part(slots),
            whole(count, units),
            part(units),
        ],
        out_specs=[part(count // 2)] * 2,
        out_shape=[jax.ShapeDtypeStruct((count // 2, features), d) for d in dtypes],
        cost_estimate=pl.CostEstimate(
            flops=2 * count * features * (2 * slots + units),
            bytes_accessed=4 * count * slots + 2 * slots * features + 4 * count * features,
            transcendentals=0,
        ),
        name="combine",
    )(high, low, back, hidden, down)


def body(
    tokens,
    routes,
    route_weights,
    norm_gain,
    gate_trained,
    up_trained,
    down_trained,
    shared_gate_trained,
    shared_up_trained,
    shared_down_trained,
):
    gr, zl, _ = (lax.axis_index(a) for a in ("gr", "zl", "y"))
    n_gr, n_zl, n_y = (lax.axis_size(a) for a in ("gr", "zl", "y"))
    n_xc = lax.axis_size("x") * lax.axis_size("c")
    n_plane = n_y * n_xc
    row_count, features = tokens.shape
    top = routes.shape[1]
    experts, own_hidden, _ = gate_trained.shape
    capacity = max(2, 3 * row_count * top // (2 * experts))

    meta = jnp.concatenate([routes.T.astype(f32), route_weights.T], axis=0)
    metas = [meta] + [swapped(meta, "zl", n_zl, k) for k in range(1, n_zl)]
    values = tokens.astype(f32)
    normed = (
        values * lax.rsqrt(jnp.mean(values * values, axis=1, keepdims=True) + epsilon)
    ).astype(bf16)
    blocks = [normed] + [swapped(normed, "zl", n_zl, k) for k in range(1, n_zl)]

    gain = norm_gain[None, :]
    shared = jnp.stack(
        [shared_gate_trained * gain, shared_up_trained * gain, shared_down_trained], axis=0
    ).astype(bf16)
    other = swapped(shared, "gr", n_gr, 1)
    shared = jnp.where(gr == 0, jnp.stack([shared, other]), jnp.stack([other, shared]))

    steps = range(n_gr * n_zl)
    place = jnp.stack([v for k in steps for v in (zl ^ (k % n_zl), gr ^ (k // n_zl))])
    place = place.astype(jnp.int32)
    sent = cast(place, norm_gain[None, :], gate_trained, up_trained, down_trained, n_plane)
    landed = plane_exchange(sent)
    piece = 3 * own_hidden

    def spread(begin, end):
        moved = [landed[:, j * piece + begin : j * piece + end] for j in range(n_zl)]
        return [moved[0]] + [
            swapped(moved[k % n_zl], ("gr", "zl"), n_gr * n_zl, k) for k in steps[1:]
        ]

    first_parts = spread(0, 2 * own_hidden)
    down_parts = spread(2 * own_hidden, piece)

    first = zl * n_plane
    near_picks = selection(metas[:2], first, n_plane, top, capacity)
    far_picks = selection(metas[2:], first, n_plane, top, capacity)

    def dispatched(code, rows, after):
        out = pick(code, *rows, 2 * capacity, 256)
        out, _ = lax.optimization_barrier((out, after))
        return plane_exchange(out.reshape(n_plane, 2 * capacity, features))

    near_in = dispatched(near_picks[0], blocks[:2], landed)
    far_in = dispatched(far_picks[0], blocks[2:], near_in)

    laid = [shared] + [swapped(shared, ("x", "c"), n_xc, k) for k in range(1, n_xc)]
    across = (lax.axis_index("x") * lax.axis_size("c") + lax.axis_index("c"))[None]
    own = lay(across.astype(jnp.int32), laid)
    columns = [own] + [swapped(own, "y", n_y, k) for k in range(1, n_y)]
    shared_out = [own[m] for m in range(3)]

    hidden = own_hidden * n_zl * n_y
    sizes = (features, hidden, n_y, n_xc, own_hidden, 256)
    near_units, expert_gate, expert_up = assemble(
        hidden_rows, place, near_in.reshape(-1, features), first_parts, 2, *sizes
    )
    far_units = over_rows(
        hidden_rows, far_in.reshape(-1, features), (expert_gate, expert_up), hidden, 256
    )
    far_units, near_weights, far_weights = lax.optimization_barrier(
        (far_units, near_picks[1], far_picks[1])
    )
    sizes = (features, features, n_y, n_xc, own_hidden, 256)
    far_result, expert_down = assemble(down_rows, place, far_units, down_parts, 1, *sizes)
    far_back = plane_exchange(far_result.reshape(n_plane, 2 * capacity, features))
    near_result = over_rows(down_rows, near_units, (expert_down,), features, 256)
    near_back = plane_exchange(near_result.reshape(n_plane, 2 * capacity, features))

    columns, _ = lax.optimization_barrier((columns, far_result))
    near_units, far_units, shared_down = shared_units(blocks, columns)
    far_back = far_back.reshape(-1, features)
    near_back = near_back.reshape(-1, features)

    third, fourth = combine(far_weights, far_back, far_units, shared_down, (bf16, bf16), 512)
    third = swapped(third, "zl", n_zl, 2)
    fourth = swapped(fourth, "zl", n_zl, 3)
    kept, second = combine(near_weights, near_back, near_units, shared_down, (f32, bf16), 512)
    second = swapped(second, "zl", n_zl, 1)
    combined = (
        kept + second.astype(f32) + third.astype(f32) + fourth.astype(f32)
    ).astype(bf16)
    return (combined, expert_gate, expert_up, expert_down, *shared_out)


def solution(mesh):
    fine = Mesh(mesh.devices.reshape(2, 4, 4, 4, 2), ALL)
    cols = ("gr", "x", "c")
    in_specs = (
        P(ALL, None),
        P(ALL, None),
        P(ALL, None),
        P(cols),
        P(None, ("zl", "y"), cols),
        P(None, ("zl", "y"), cols),
        P(None, ("zl", "y"), cols),
        P(("zl", "y"), cols),
        P(("zl", "y"), cols),
        P(("zl", "y"), cols),
    )
    out_specs = (
        P(ALL, None),
        P(("zl", "y", "x", "c"), None, None),
        P(("zl", "y", "x", "c"), None, None),
        P(("zl", "y", "x", "c"), None, None),
        P(("zl", "y"), None),
        P(("zl", "y"), None),
        P(("zl", "y"), None),
    )

    def step(*args):
        return body(*args)

    step = jax.shard_map(step, mesh=fine, in_specs=in_specs, out_specs=out_specs, check_vma=False)
    return step
```

```python
import functools

import jax
import jax.numpy as jnp
from jax import lax
from jax.experimental import pallas as pl
from jax.experimental.pallas import tpu as pltpu
from jax.sharding import Mesh, PartitionSpec as P


epsilon = 1e-06
ALL = ("gr", "zl", "y", "x", "c")
PLANE = ("y", "x", "c")
bf16 = jnp.bfloat16
f32 = jnp.float32


def swapped(array, axis, size, k):
    return lax.ppermute(array, axis, [(r, r ^ k) for r in range(size)])


def plane_exchange(array):
    return lax.all_to_all(array, PLANE, split_axis=0, concat_axis=0, tiled=True)


def cast_kernel(place, gain, gate, up, down, out):
    n = gate.shape[1]
    scale = gain[...][None]
    out[:, :n, :] = (gate[...] * scale).astype(bf16)
    out[:, n : 2 * n, :] = (up[...] * scale).astype(bf16)
    out[:, 2 * n :, :] = down[...].astype(bf16)


def cast(place, gain, gate, up, down, n_plane):
    experts, n, cols = gate.shape
    n_zl = experts // n_plane
    piece = pl.BlockSpec((n_plane, n, cols), lambda j, p: (p[0] ^ j, 0, 0))
    spec = pltpu.PrefetchScalarGridSpec(
        num_scalar_prefetch=1,
        grid=(n_zl,),
        in_specs=[pl.BlockSpec((1, cols), lambda j, p: (0, 0)), piece, piece, piece],
        out_specs=pl.BlockSpec((n_plane, 3 * n, cols), lambda j, p: (0, j, 0)),
    )
    return pl.pallas_call(
        cast_kernel,
        grid_spec=spec,
        out_shape=jax.ShapeDtypeStruct((n_plane, n_zl * 3 * n, cols), bf16),
        cost_estimate=pl.CostEstimate(
            flops=3 * gate.size, bytes_accessed=18 * gate.size, transcendentals=0
        ),
        name="cast",
    )(place, gain, gate, up, down)


def hidden_rows(x, gate, up):
    contract = (((1,), (1,)), ((), ()))
    g = lax.dot_general(x, gate, contract, preferred_element_type=f32)
    u = lax.dot_general(x, up, contract, preferred_element_type=f32)
    return (jax.nn.silu(g) * u).astype(bf16)


def down_rows(hidden, down):
    return jnp.dot(hidden, down, preferred_element_type=f32).astype(bf16)


def assemble_kernel(place, x, *refs, compute, blocks, matrices, n_y, n_xc, own_hidden, cols):
    parts, refs = refs[:blocks], refs[blocks:]
    out, outs, held, sems = refs[0], refs[1 : 1 + matrices], refs[1 + matrices : -1], refs[-1]
    step = pl.program_id(0)
    n_cols = held[0].shape[0]

    def writes():
        return [
            pltpu.make_async_copy(
                held[m].at[f],
                outs[m].at[0, :, pl.ds(f * cols, cols)],
                sems.at[blocks * matrices * n_y + m * n_cols + f],
            )
            for m in range(matrices)
            for f in range(n_cols)
        ]

    @pl.when(step == 0)
    def _():
        reads = []
        for k in range(blocks):
            row = place[2 * k] * (n_y * own_hidden)
            col = place[2 * k + 1] * n_xc
            for m in range(matrices):
                for y in range(n_y):
                    at = pl.multiple_of(row + y * own_hidden, 8)
                    reads.append(
                        pltpu.make_async_copy(
                            parts[k].at[pl.ds(y * n_xc, n_xc), pl.ds(m * own_hidden, own_hidden)],
                            held[m].at[pl.ds(col, n_xc), pl.ds(at, own_hidden)],
                            sems.at[(k * matrices + m) * n_y + y],
                        )
                    )
        for r in reads:
            r.start()
        for r in reads:
            r.wait()
        for w in writes():
            w.start()

    whole = [jnp.concatenate([h[f] for f in range(n_cols)], axis=1) for h in held]
    out[...] = compute(x[...], *whole)

    @pl.when(step == pl.num_programs(0) - 1)
    def _():
        for w in writes():
            w.wait()


def assemble(compute, place, x, parts, matrices, features, width, n_y, n_xc, own_hidden, tile):
    count, depth = x.shape
    cols = parts[0].shape[2]
    n_cols = features // cols
    hidden = len(parts) * n_y * n_xc * own_hidden * cols // features
    matrix = jax.ShapeDtypeStruct((1, hidden, features), bf16)
    hbm = pl.BlockSpec(memory_space=pl.ANY)
    spec = pltpu.PrefetchScalarGridSpec(
        num_scalar_prefetch=1,
        grid=(count // tile,),
        in_specs=[pl.BlockSpec((tile, depth), lambda i, p: (i, 0))] + [hbm] * len(parts),
        out_specs=[pl.BlockSpec((tile, width), lambda i, p: (i, 0))] + [hbm] * matrices,
        scratch_shapes=[pltpu.VMEM((n_cols, hidden, cols), bf16)] * matrices
        + [pltpu.SemaphoreType.DMA((len(parts) * matrices * n_y + matrices * n_cols,))],
    )
    return pl.pallas_call(
        functools.partial(
            assemble_kernel,
            compute=compute,
            blocks=len(parts),
            matrices=matrices,
            n_y=n_y,
            n_xc=n_xc,
            own_hidden=own_hidden,
            cols=cols,
        ),
        grid_spec=spec,
        out_shape=[jax.ShapeDtypeStruct((count, width), bf16)] + [matrix] * matrices,
        cost_estimate=pl.CostEstimate(
            flops=2 * matrices * count * hidden * features,
            bytes_accessed=4 * count * features + 4 * matrices * hidden * features,
            transcendentals=count * hidden,
        ),
        name="assemble",
    )(place, x, *parts)


def rows_kernel(x, *refs, compute):
    refs[-1][...] = compute(x[...], *(r[0] for r in refs[:-1]))


def over_rows(compute, x, matrices, width, tile):
    count, depth = x.shape
    whole = pl.BlockSpec(matrices[0].shape, lambda i: (0, 0, 0))
    return pl.pallas_call(
        functools.partial(rows_kernel, compute=compute),
        grid=(count // tile,),
        in_specs=[pl.BlockSpec((tile, depth), lambda i: (i, 0))] + [whole] * len(matrices),
        out_specs=pl.BlockSpec((tile, width), lambda i: (i, 0)),
        out_shape=jax.ShapeDtypeStruct((count, width), bf16),
        cost_estimate=pl.CostEstimate(
            flops=2 * count * sum(m.size for m in matrices),
            bytes_accessed=2 * count * (depth + width) + 2 * sum(m.size for m in matrices),
            transcendentals=count,
        ),
        name="over_rows",
    )(x, *matrices)


def selection(metas, first, experts, top, capacity):
    span = len(metas) * capacity
    slot = jnp.arange(experts * span, dtype=jnp.int32)
    within = (slot % span).astype(f32)
    spread = (slot[:, None] // span == jnp.arange(experts, dtype=jnp.int32)[None, :]).astype(bf16)

    def by_token(values):
        return lax.dot_general(
            values, spread, (((0,), (1,)), ((), ())), preferred_element_type=f32
        )

    codes, weights = [], []
    for k, meta in enumerate(metas):
        names = meta[:top] - first.astype(f32)
        hits = names[:, None, :] == jnp.arange(experts, dtype=f32)[None, :, None]
        chosen = jnp.sum(hits.astype(f32), axis=0)
        weight = jnp.sum(jnp.where(hits, meta[top:, None, :], 0.0), axis=0)
        n = chosen.shape[1]
        before = (jnp.arange(n)[:, None] < jnp.arange(n)[None, :]).astype(bf16)
        place = jnp.dot(chosen.astype(bf16), before, preferred_element_type=f32)
        codes.append(jnp.where(chosen > 0, place + float(k * capacity), -1.0))
        weights.append(weight)
    code = jnp.concatenate(codes, axis=1).astype(bf16)
    weight = jnp.concatenate(weights, axis=1)
    high = weight.astype(bf16)
    low = (weight - high.astype(f32)).astype(bf16)
    held = by_token(code) == within[None, :]
    high = jnp.where(held, by_token(high), 0.0).astype(bf16)
    low = jnp.where(held, by_token(low), 0.0).astype(bf16)
    return code, (high, low)


def pick_kernel(code, one, two, out, *, span, tile):
    slot = lax.broadcasted_iota(jnp.int32, (tile, 1), 0) + pl.program_id(0) * tile
    expert = slot // span
    within = (slot - expert * span).astype(f32)
    names = lax.broadcasted_iota(jnp.int32, (tile, code.shape[0]), 1)
    spread = (names == expert).astype(f32).astype(bf16)
    held = jnp.dot(spread, code[...], preferred_element_type=f32) == within
    held = held.astype(f32).astype(bf16)
    n = one.shape[0]
    total = jnp.dot(held[:, :n], one[...], preferred_element_type=f32)
    total += jnp.dot(held[:, n:], two[...], preferred_element_type=f32)
    out[...] = total.astype(bf16)


def pick(code, one, two, span, tile):
    experts, count = code.shape
    features = one.shape[1]
    slots = experts * span
    whole = lambda a: pl.BlockSpec(a.shape, lambda i: (0, 0))
    return pl.pallas_call(
        functools.partial(pick_kernel, span=span, tile=tile),
        grid=(slots // tile,),
        in_specs=[whole(code), whole(one), whole(two)],
        out_specs=pl.BlockSpec((tile, features), lambda i: (i, 0)),
        out_shape=jax.ShapeDtypeStruct((slots, features), bf16),
        cost_estimate=pl.CostEstimate(
            flops=2 * slots * count * features,
            bytes_accessed=2 * (slots + count) * features,
            transcendentals=0,
        ),
        name="pick",
    )(code, one, two)


def lay_kernel(place, *refs):
    pieces, out, held = refs[:-2], refs[-2], refs[-1]
    n = len(pieces)
    groups, _, _, cols = pieces[0].shape
    for k in range(n):
        for g in range(groups):
            held[g * n + (k ^ place[0])] = pieces[k][g]
    for f in range(groups * n):
        out[:, :, f * cols : (f + 1) * cols] = held[f]


def lay(place, pieces):
    n = len(pieces)
    groups, matrices, rows, cols = pieces[0].shape
    piece = pl.BlockSpec(pieces[0].shape, lambda i, p: (0,) * 4)
    spec = pltpu.PrefetchScalarGridSpec(
        num_scalar_prefetch=1,
        grid=(1,),
        in_specs=[piece] * n,
        out_specs=pl.BlockSpec((matrices, rows, groups * n * cols), lambda i, p: (0, 0, 0)),
        scratch_shapes=[pltpu.VMEM((groups * n, matrices, rows, cols), bf16)],
    )
    return pl.pallas_call(
        lay_kernel,
        grid_spec=spec,
        out_shape=jax.ShapeDtypeStruct((matrices, rows, groups * n * cols), bf16),
        cost_estimate=pl.CostEstimate(
            flops=n * pieces[0].size, bytes_accessed=4 * n * pieces[0].size, transcendentals=0
        ),
        name="lay",
    )(place, *pieces)


def units_kernel(*refs, blocks):
    tokens, refs = refs[:blocks], refs[blocks:]
    columns, (near, far, down) = refs[:-3], refs[-3:]
    gate, up, last = (jnp.concatenate([c[m] for c in columns], axis=0) for m in range(3))
    down[...] = last
    half = blocks // 2
    for out, pair in ((near, tokens[:half]), (far, tokens[half:])):
        rows = jnp.concatenate([t[...] for t in pair], axis=0)
        out[...] = hidden_rows(rows, gate, up)


def shared_units(tokens, columns):
    count, features = tokens[0].shape
    units = len(columns) * columns[0].shape[1]
    half = len(tokens) // 2 * count
    return pl.pallas_call(
        functools.partial(units_kernel, blocks=len(tokens)),
        out_shape=[jax.ShapeDtypeStruct((half, units), bf16)] * 2
        + [jax.ShapeDtypeStruct((units, features), bf16)],
        cost_estimate=pl.CostEstimate(
            flops=8 * half * units * features,
            bytes_accessed=4 * half * features + 8 * units * features,
            transcendentals=2 * half * units,
        ),
        name="shared_units",
    )(*tokens, *columns)


def combine_kernel(high, low, back, hidden, down, one, two):
    rows = back[...]
    total = jnp.dot(high[...], rows, preferred_element_type=f32)
    total += jnp.dot(low[...], rows, preferred_element_type=f32)
    total += jnp.dot(hidden[...], down[...], preferred_element_type=f32)
    n = one.shape[0]
    one[...] = total[:n].astype(one.dtype)
    two[...] = total[n:].astype(two.dtype)


def combine(weights, back, hidden, down, dtypes, tile):
    high, low = weights
    count, slots = high.shape
    features = back.shape[1]
    units = hidden.shape[1]
    whole = lambda *shape: pl.BlockSpec(shape, lambda i: (0, 0))
    part = lambda rows: pl.BlockSpec((rows, tile), lambda i: (0, i))
    return pl.pallas_call(
        combine_kernel,
        grid=(features // tile,),
        in_specs=[
            whole(count, slots),
            whole(count, slots),
            part(slots),
            whole(count, units),
            part(units),
        ],
        out_specs=[part(count // 2)] * 2,
        out_shape=[jax.ShapeDtypeStruct((count // 2, features), d) for d in dtypes],
        cost_estimate=pl.CostEstimate(
            flops=2 * count * features * (2 * slots + units),
            bytes_accessed=4 * count * slots + 2 * slots * features + 4 * count * features,
            transcendentals=0,
        ),
        name="combine",
    )(high, low, back, hidden, down)


def body(
    tokens,
    routes,
    route_weights,
    norm_gain,
    gate_trained,
    up_trained,
    down_trained,
    shared_gate_trained,
    shared_up_trained,
    shared_down_trained,
):
    gr, zl, _ = (lax.axis_index(a) for a in ("gr", "zl", "y"))
    n_gr, n_zl, n_y = (lax.axis_size(a) for a in ("gr", "zl", "y"))
    n_xc = lax.axis_size("x") * lax.axis_size("c")
    n_plane = n_y * n_xc
    row_count, features = tokens.shape
    top = routes.shape[1]
    experts, own_hidden, _ = gate_trained.shape
    capacity = max(2, 3 * row_count * top // (2 * experts))

    meta = jnp.concatenate([routes.T.astype(f32), route_weights.T], axis=0)
    metas = [meta] + [swapped(meta, "zl", n_zl, k) for k in range(1, n_zl)]
    values = tokens.astype(f32)
    normed = (
        values * lax.rsqrt(jnp.mean(values * values, axis=1, keepdims=True) + epsilon)
    ).astype(bf16)
    blocks = [normed] + [swapped(normed, "zl", n_zl, k) for k in range(1, n_zl)]

    gain = norm_gain[None, :]
    shared = jnp.stack(
        [shared_gate_trained * gain, shared_up_trained * gain, shared_down_trained], axis=0
    ).astype(bf16)
    other = swapped(shared, "gr", n_gr, 1)
    shared = jnp.where(gr == 0, jnp.stack([shared, other]), jnp.stack([other, shared]))

    steps = range(n_gr * n_zl)
    place = jnp.stack([v for k in steps for v in (zl ^ (k % n_zl), gr ^ (k // n_zl))])
    place = place.astype(jnp.int32)
    sent = cast(place, norm_gain[None, :], gate_trained, up_trained, down_trained, n_plane)
    landed = plane_exchange(sent)
    piece = 3 * own_hidden

    def spread(begin, end):
        moved = [landed[:, j * piece + begin : j * piece + end] for j in range(n_zl)]
        return [moved[0]] + [
            swapped(moved[k % n_zl], ("gr", "zl"), n_gr * n_zl, k) for k in steps[1:]
        ]

    first_parts = spread(0, 2 * own_hidden)
    down_parts = spread(2 * own_hidden, piece)

    first = zl * n_plane
    near_picks = selection(metas[:2], first, n_plane, top, capacity)
    far_picks = selection(metas[2:], first, n_plane, top, capacity)

    def dispatched(code, rows, after):
        out = pick(code, *rows, 2 * capacity, 256)
        out, _ = lax.optimization_barrier((out, after))
        return plane_exchange(out.reshape(n_plane, 2 * capacity, features))

    near_in = dispatched(near_picks[0], blocks[:2], landed)
    far_in = dispatched(far_picks[0], blocks[2:], near_in)

    laid = [shared] + [swapped(shared, ("x", "c"), n_xc, k) for k in range(1, n_xc)]
    across = (lax.axis_index("x") * lax.axis_size("c") + lax.axis_index("c"))[None]
    own = lay(across.astype(jnp.int32), laid)
    columns = [own] + [swapped(own, "y", n_y, k) for k in range(1, n_y)]
    shared_out = [own[m] for m in range(3)]

    hidden = own_hidden * n_zl * n_y
    sizes = (features, hidden, n_y, n_xc, own_hidden, 256)
    near_units, expert_gate, expert_up = assemble(
        hidden_rows, place, near_in.reshape(-1, features), first_parts, 2, *sizes
    )
    far_units = over_rows(
        hidden_rows, far_in.reshape(-1, features), (expert_gate, expert_up), hidden, 256
    )
    far_units, near_weights, far_weights = lax.optimization_barrier(
        (far_units, near_picks[1], far_picks[1])
    )
    sizes = (features, features, n_y, n_xc, own_hidden, 256)
    far_result, expert_down = assemble(down_rows, place, far_units, down_parts, 1, *sizes)
    far_back = plane_exchange(far_result.reshape(n_plane, 2 * capacity, features))
    near_result = over_rows(down_rows, near_units, (expert_down,), features, 256)
    near_back = plane_exchange(near_result.reshape(n_plane, 2 * capacity, features))

    columns, _ = lax.optimization_barrier((columns, far_result))
    near_units, far_units, shared_down = shared_units(blocks, columns)
    far_back = far_back.reshape(-1, features)
    near_back = near_back.reshape(-1, features)

    across, beside = combine(far_weights, far_back, far_units, shared_down, (f32, bf16), 512)
    beside = swapped(beside, "zl", n_zl, 1)
    across = (across + beside.astype(f32)).astype(bf16)
    across = swapped(across, "zl", n_zl, 2)
    kept, second = combine(near_weights, near_back, near_units, shared_down, (f32, bf16), 512)
    second = swapped(second, "zl", n_zl, 1)
    combined = (
        kept + second.astype(f32) + across.astype(f32)
    ).astype(bf16)
    return (combined, expert_gate, expert_up, expert_down, *shared_out)


def solution(mesh):
    fine = Mesh(mesh.devices.reshape(2, 4, 4, 4, 2), ALL)
    cols = ("gr", "x", "c")
    in_specs = (
        P(ALL, None),
        P(ALL, None),
        P(ALL, None),
        P(cols),
        P(None, ("zl", "y"), cols),
        P(None, ("zl", "y"), cols),
        P(None, ("zl", "y"), cols),
        P(("zl", "y"), cols),
        P(("zl", "y"), cols),
        P(("zl", "y"), cols),
    )
    out_specs = (
        P(ALL, None),
        P(("zl", "y", "x", "c"), None, None),
        P(("zl", "y", "x", "c"), None, None),
        P(("zl", "y", "x", "c"), None, None),
        P(("zl", "y"), None),
        P(("zl", "y"), None),
        P(("zl", "y"), None),
    )

    def step(*args):
        return body(*args)

    step = jax.shard_map(step, mesh=fine, in_specs=in_specs, out_specs=out_specs, check_vma=False)
    return step
```
